256 devices in a mesh: ep: 64 (over z, y, core), tp: 4 (over x).
Axes of the slice: x: 4, y: 4, z: 8, core: 2. Of those that a mesh axis runs over, the one named last changes fastest.
Arguments:
- tokens: bfloat16 [1024, 2048], P('ep'), may hold values from -6 to 6
- key_cache: bfloat16 [1024, 1024, 512], P('ep', None, 'tp'), may hold values from -6 to 6
- value_cache: bfloat16 [1024, 1024, 512], P('ep', None, 'tp'), may hold values from -6 to 6
- lengths: int32 [1024], P('ep'), may hold values from 1 to 1024, as said below
- attn_gain: float32 [2048], replicated, may hold values from 0.1 to 1.9
- query_weight: bfloat16 [2048, 1024], P('ep', 'tp'), may hold values from -0.125 to 0.125
- key_weight: bfloat16 [2048, 512], P('ep', 'tp'), may hold values from -0.125 to 0.125
- value_weight: bfloat16 [2048, 512], P('ep', 'tp'), may hold values from -0.125 to 0.125
- stay_bias: float32 [8], P('tp'), may hold values from -7.5 to -4
- out_weight: bfloat16 [1024, 2048], P('tp'), may hold values from -4 to 4
- ffn_gain: float32 [2048], replicated, may hold values from 0.1 to 1.9
- gate_weight: bfloat16 [64, 2048, 1024], P('ep', None, 'tp')
- up_weight: bfloat16 [64, 2048, 1024], P('ep', None, 'tp')
- down_weight: bfloat16 [64, 1024, 2048], P('ep', 'tp'), may hold values from -0.0234375 to 0.0234375
- routes: int32 [1024, 4], P('ep'), may hold values from 0 to 63, as said below
- route_weight: float32 [1024, 4], P('ep'), may hold values from 0.05 to 1
Outputs:
- layer_out: bfloat16 [1024, 2048], P('ep', 'tp')
- new_keys: bfloat16 [1024, 512], P('ep', 'tp')
- new_values: bfloat16 [1024, 512], P('ep', 'tp')
The draws below stay inside these ranges and needn't reach their ends.
Inputs may be any that keep to these rules, and one draw needn't show every extreme that they name: `lengths`: the sequences of every index of ep include one with length 1024. `routes`: each row names 4 different experts; the rows of one device (aligned blocks of 16 rows) name any one expert at most 2 times; in every draw one expert is named exactly 2 times by the rows of every device.
All inputs are finite; a program needn't handle non-finite values.
Results may differ from the reference program's by a relative error of at most 0.018.
Values may be sent and summed in bfloat16 or wider, within the bound.
A program may use at most 64 MiB of HBM per device.

```python
import math
import jax
import jax.numpy as jnp
from jax import lax

D = 2048
HQ = 8
KVH = 4
HD = 128
FF = 1024
TOPK = 4
SEQS = 16
CACHE = 1024
EXPERTS = 64
BATCH = 1024
CAP = 2
N_EP = 64
N_TP = 4


def draw_lengths(key, part):
    groups = BATCH // SEQS
    first_key, second_key = jax.random.split(jax.random.fold_in(key, 3))
    spread = jax.random.randint(first_key, (BATCH,), 1, CACHE + 1)
    longest = jax.random.randint(second_key, (groups,), 0, SEQS)
    row_ids = jnp.arange(BATCH, dtype=jnp.int32)
    return jnp.where(row_ids % SEQS == longest[row_ids // SEQS], CACHE, spread).astype(jnp.int32)


def draw_routes(key, part):
    groups = BATCH // SEQS
    subkeys = jax.random.split(jax.random.fold_in(key, 5), 4)
    favoured = jax.random.randint(subkeys[0], (), 0, EXPERTS)
    leaning = jax.random.randint(subkeys[1], (EXPERTS,), 0, 4)
    jitter = jax.random.randint(subkeys[2], (groups, SEQS, EXPERTS), 0, 65536)
    expert_ids = jnp.arange(EXPERTS, dtype=jnp.int32)

    def one_block(block_jitter):

        def assign_row(counts, row_jitter):
            score = (row_jitter + leaning * 65536) * EXPERTS + expert_ids
            score = score + jnp.where((expert_ids == favoured) & (counts < CAP), 1 << 28, 0)
            score = jnp.where(counts >= CAP, score - (1 << 29), score)
            chosen = lax.top_k(score, TOPK)[1].astype(jnp.int32)
            counts = counts + jnp.sum((chosen[:, None] == expert_ids[None, :]).astype(jnp.int32), axis=0)
            return (counts, chosen)
        return lax.scan(assign_row, jnp.zeros((EXPERTS,), jnp.int32), block_jitter)[1]
    picked = jax.vmap(one_block)(jitter)
    orders = jax.vmap(lambda sub_key: jax.random.permutation(sub_key, SEQS))(jax.random.split(subkeys[3], groups))
    picked = jnp.take_along_axis(picked, orders[:, :, None].astype(jnp.int32), axis=1)
    return picked.reshape(BATCH, TOPK).astype(jnp.int32)


def scaled_columns(key, lowest, highest):
    first_key, second_key = jax.random.split(key)
    spread = jax.random.uniform(first_key, (EXPERTS, 1, FF), jnp.float32, math.log(lowest), math.log(highest))
    values = jnp.clip(jax.random.normal(second_key, (EXPERTS, D, FF), jnp.float32), -6.0, 6.0)
    return (values * jnp.exp(spread) * D ** (-0.5)).astype(jnp.bfloat16)


def draw_gate_weight(key, part):
    return scaled_columns(jax.random.fold_in(key, 7), 0.5, 9.0)


def draw_up_weight(key, part):
    return scaled_columns(jax.random.fold_in(key, 13), 0.5, 9.0)


def block_levels(own_key, dims, cuts, smallest, largest):
    def one(axis_at, shards_of):
        draws = jax.random.uniform(jax.random.fold_in(jax.random.fold_in(own_key, 6), axis_at), (shards_of,), jnp.float32, smallest / len(cuts), largest / len(cuts))
        return jnp.repeat(jnp.exp(draws), dims[axis_at] // shards_of).reshape((-1,) + (1,) * (len(dims) - axis_at - 1))

    factor_of = one(*cuts[0])
    for cut in cuts[1:]:
        factor_of = factor_of * one(*cut)
    return factor_of


def centred(key, dims, scale, most, cuts=(), kind=jnp.bfloat16):
    values = jax.random.normal(key, dims, jnp.float32) * scale
    if len(cuts) > 0:
        values = block_levels(key, dims, cuts, -0.22, 0.18) * values
    return jnp.clip(values, min=-most, max=most).astype(kind)


def setup_inputs(seed: int = 0) -> dict:
    seeds = jax.random.split(jax.random.key(seed), 17)
    tokens = centred(seeds[0], (BATCH, D), 1.0, 6.0, ((0, 64),))
    key_cache = centred(seeds[1], (BATCH, CACHE, KVH * HD), 1.0, 6.0, ((0, 64), (2, 4)))
    value_cache = centred(seeds[2], (BATCH, CACHE, KVH * HD), 1.0, 6.0, ((0, 64), (2, 4)))
    lengths = draw_lengths(jax.random.fold_in(seeds[16], 71), 0)
    attn_gain = jnp.clip(1.0 + 0.18 * jax.random.normal(seeds[4], (D,), jnp.float32), 0.1, 1.9)
    query_weight = centred(seeds[5], (D, HQ * HD), D ** -0.5, 0.125, ((0, 64), (1, 4)))
    key_weight = centred(seeds[6], (D, KVH * HD), D ** -0.5, 0.125, ((0, 64), (1, 4)))
    value_weight = centred(seeds[7], (D, KVH * HD), D ** -0.5, 0.125, ((0, 64), (1, 4)))
    stay_bias = jnp.clip(-7.5 + 3.5 * jax.random.uniform(seeds[8], (HQ,), jnp.float32) ** block_levels(seeds[8], (HQ,), ((0, 4),), -0.2, 0.2), -7.5, -4.0)
    out_weight = centred(seeds[9], (HQ * HD, D), 0.25, 4.0, ((0, 4),))
    ffn_gain = jnp.clip(1.0 + 0.18 * jax.random.normal(seeds[10], (D,), jnp.float32), 0.1, 1.9)
    gate_weight = draw_gate_weight(jax.random.fold_in(seeds[16], 71), 0)
    up_weight = draw_up_weight(jax.random.fold_in(seeds[16], 71), 0)
    down_weight = centred(seeds[13], (EXPERTS, FF, D), (64 * FF) ** -0.5, 0.0234375, ((0, 64), (1, 4)))
    routes = draw_routes(jax.random.fold_in(seeds[16], 71), 0)
    route_weight = jnp.clip(0.05 + 0.95 * jax.random.uniform(seeds[15], (BATCH, TOPK), jnp.float32) ** block_levels(seeds[15], (BATCH, TOPK), ((0, 64),), -0.2, 0.2), 0.05, 1.0)
    return dict(tokens=tokens, key_cache=key_cache, value_cache=value_cache, lengths=lengths, attn_gain=attn_gain, query_weight=query_weight, key_weight=key_weight, value_weight=value_weight, stay_bias=stay_bias, out_weight=out_weight, ffn_gain=ffn_gain, gate_weight=gate_weight, up_weight=up_weight, down_weight=down_weight, routes=routes, route_weight=route_weight)


eps_norm = 1e-05
clamp_limit = 7.0
gate_alpha = 1.702

def rms_scale(values, gain):
    floats = values.astype(jnp.float32)
    scaled = floats * lax.rsqrt(lax.optimization_barrier(jnp.mean(floats * floats, axis=-1, keepdims=True)) + eps_norm)
    return scaled * gain.astype(jnp.float32)

def stick_weights(scores, live_mask):
    log_stay = jnp.where(live_mask, jax.nn.log_sigmoid(-scores), 0.0)
    later_sum = lax.cumsum(log_stay, axis=scores.ndim - 1, reverse=True) - log_stay
    return jnp.where(live_mask, jnp.exp(jax.nn.log_sigmoid(scores) + later_sum), 0.0)

def expert_units(gate_pre, upward):
    capped = jnp.minimum(gate_pre, clamp_limit)
    upward = jnp.clip(upward, -clamp_limit, clamp_limit)
    return capped * jax.nn.sigmoid(gate_alpha * capped) * (upward + 1.0)

def rounded_parts(head_parts):
    return lax.optimization_barrier(head_parts.astype(jnp.bfloat16)).astype(jnp.float32).sum(axis=0)

def reference(tokens, key_cache, value_cache, lengths, attn_gain, query_weight, key_weight, value_weight, stay_bias, out_weight, ffn_gain, gate_weight, up_weight, down_weight, routes, route_weight):
    normed = rms_scale(tokens, attn_gain).astype(jnp.bfloat16)
    queries = jnp.dot(normed, query_weight, preferred_element_type=jnp.float32).astype(jnp.bfloat16)
    new_keys = jnp.dot(normed, key_weight, preferred_element_type=jnp.float32).astype(jnp.bfloat16)
    new_values = jnp.dot(normed, value_weight, preferred_element_type=jnp.float32).astype(jnp.bfloat16)
    group_size = HQ // KVH
    head_bias = stay_bias.astype(jnp.float32).reshape(KVH, group_size, 1)
    positions = jnp.arange(CACHE, dtype=jnp.int32)

    def attend_one(inputs):
        query_row, key_rows, value_rows, length = inputs
        grouped = query_row.reshape(KVH, group_size, HD).astype(jnp.float32)
        keyed = key_rows.reshape(CACHE, KVH, HD).astype(jnp.float32)
        scores = jnp.einsum('kgd,ckd->kgc', grouped, keyed) * HD ** (-0.5) + head_bias
        live_mask = (positions < length)[None, None, :]
        weights = lax.optimization_barrier(stick_weights(scores, live_mask).astype(jnp.bfloat16))
        valued = value_rows.reshape(CACHE, KVH, HD).astype(jnp.float32)
        mixed_rows = jnp.einsum('kgc,ckd->kgd', weights.astype(jnp.float32), valued)
        return mixed_rows.astype(jnp.bfloat16).reshape(HQ * HD)
    attended = lax.map(attend_one, (queries, key_cache, value_cache, lengths))
    head_parts = jnp.einsum('btj,tjd->tbd', attended.reshape(BATCH, N_TP, -1).astype(jnp.float32), out_weight.reshape(N_TP, -1, D).astype(jnp.float32))
    residual = (tokens.astype(jnp.float32) + rounded_parts(head_parts)).astype(jnp.bfloat16)
    ffn_in = rms_scale(residual, ffn_gain).astype(jnp.bfloat16)
    pair_count = BATCH * TOPK
    most_rows = N_EP * CAP
    flat_routes = routes.reshape(-1)
    flat_weight = jnp.concatenate([route_weight.reshape(-1), jnp.zeros((1,), jnp.float32)])
    padded_in = jnp.concatenate([ffn_in, jnp.zeros((1, D), jnp.bfloat16)], axis=0)

    def one_expert(accumulated, expert):
        chosen = jnp.nonzero(flat_routes == expert, size=most_rows, fill_value=pair_count)[0].astype(jnp.int32)
        token_rows = chosen // TOPK
        picked_rows = padded_in[token_rows]
        gate_pre = jnp.dot(picked_rows, gate_weight[expert], preferred_element_type=jnp.float32)
        upward = jnp.dot(picked_rows, up_weight[expert], preferred_element_type=jnp.float32)
        unit_out = expert_units(gate_pre, upward).astype(jnp.bfloat16)
        expert_parts = jnp.einsum('rtf,tfd->trd', unit_out.reshape(most_rows, N_TP, -1).astype(jnp.float32), down_weight[expert].reshape(N_TP, -1, D).astype(jnp.float32))
        expert_out = rounded_parts(expert_parts).astype(jnp.bfloat16)
        weighted = flat_weight[chosen][:, None] * expert_out.astype(jnp.float32)
        return (accumulated.at[token_rows].add(weighted), None)
    accumulated, _ = lax.scan(one_expert, jnp.zeros((BATCH + 1, D), jnp.float32), jnp.arange(EXPERTS, dtype=jnp.int32))
    layer_out = (residual.astype(jnp.float32) + accumulated[:BATCH]).astype(jnp.bfloat16)
    return (layer_out, new_keys, new_values)
```

```python
import functools
import math

import jax
import jax.numpy as jnp
from jax import lax
from jax.experimental import pallas as pl
from jax.experimental.pallas import tpu as pltpu
from jax.sharding import Mesh
from jax.sharding import PartitionSpec as P

AXES = ("ep_0", "ep_1", "ep_2", "tp")
EP = AXES[:3]
MESH = pl.DeviceIdType.MESH
F32 = jnp.float32
BF16 = jnp.bfloat16
HD = 128
CAP = 2
eps_norm = 1e-05
clamp_limit = 7.0
gate_alpha = 1.702


def dot(a, b, dims=((1,), (0,))):
    return lax.dot_general(a, b, (dims, ((), ())), preferred_element_type=F32)


def rms_scale(values, gain):
    scale = lax.rsqrt(jnp.mean(values * values, axis=-1, keepdims=True) + eps_norm)
    return values * scale * gain


def iota(shape, dim):
    return lax.broadcasted_iota(jnp.int32, shape, dim)


def layer_kernel(
    sizes,
    tokens, key_cache, value_cache, lengths, attn_gain, query_weight, key_weight, value_weight,
    stay_bias, out_weight, ffn_gain, gate_weight, up_weight, down_weight, routes, route_weight,
    layer_out, new_keys, new_values,
    tok, gain_a, gain_f, route_v, rweight_v, kc, vc, ow, gw, uw, dw,
    normed, slices, wq, wkv, part_q, part_kv, got_q, got_kv,
    sticks, hp, hr, sb, xg, epart, egot, rb, rt,
    loc, kv_sem, exp_sem, send, recv, chunk_recv, group_recv, group_got,
):
    NZ, NY, NC, NX = sizes
    NP = NY * NC
    NE = NZ * NP
    z, y, c, x = (lax.axis_index(a) for a in AXES)
    yc = y * NC + c
    me = z * NP + yc
    seqs, width = tok.shape
    kblock = width // NZ
    quarter = width // NX
    QB = quarter // HD
    cache_len = kc.shape[1]
    RB = CAP * QB
    topk = route_v.shape[1]

    def zplus(d):
        return lax.rem(z + d, NZ)

    def pplus(i):
        j = lax.rem(yc + i, NP)
        return j, {"ep_1": j // NC, "ep_2": lax.rem(j, NC)}

    def xplus(d):
        return lax.rem(x + d, NX)

    barrier = pltpu.get_barrier_semaphore()
    for d in range(1, NZ):
        pl.semaphore_signal(barrier, inc=1, device_id={"ep_0": zplus(d)}, device_id_type=MESH)
    for i in range(1, NP):
        pl.semaphore_signal(barrier, inc=1, device_id=pplus(i)[1], device_id_type=MESH)
    for d in range(1, NX):
        pl.semaphore_signal(barrier, inc=1, device_id={"tp": xplus(d)}, device_id_type=MESH)

    def load(src, dst, sem):
        copy = pltpu.make_async_copy(src, dst, sem)
        copy.start()
        return copy

    ld_tok = load(tokens, tok, loc.at[0])
    ld_ga = load(attn_gain, gain_a, loc.at[1])
    ld_wq = load(query_weight, wq.at[yc], loc.at[2])
    ld_wk = load(key_weight, wkv.at[yc, :, pl.ds(0, HD)], loc.at[3])
    ld_wv = load(value_weight, wkv.at[yc, :, pl.ds(HD, HD)], loc.at[4])
    ld_rt = load(routes, route_v, loc.at[5])
    ld_rw = load(route_weight, rweight_v, loc.at[6])
    ld_gf = load(ffn_gain, gain_f, loc.at[7])
    npair = seqs // 2
    ld_k = [load(key_cache.at[pl.ds(2 * p, 2)], kc.at[pl.ds(2 * p, 2)], kv_sem.at[0, p]) for p in range(npair)]
    ld_v = [load(value_cache.at[pl.ds(2 * p, 2)], vc.at[pl.ds(2 * p, 2)], kv_sem.at[1, p]) for p in range(npair)]
    ld_ow = load(out_weight, ow, exp_sem.at[0])
    ld_gw = load(gate_weight.at[0], gw, exp_sem.at[1])
    ld_uw = load(up_weight.at[0], uw, exp_sem.at[2])
    ld_dw = load(down_weight.at[0], dw, exp_sem.at[3])

    def remote(src, dst, s, r, device):
        return pltpu.make_async_remote_copy(
            src_ref=src, dst_ref=dst, send_sem=s, recv_sem=r, device_id=device, device_id_type=MESH
        )

    def wait_bytes(ref, sem):
        pltpu.make_async_copy(ref, ref, sem).wait()

    ld_tok.wait()
    ld_ga.wait()
    normed[...] = rms_scale(tok[...].astype(F32), gain_a[...]).astype(BF16)
    ld_wq.wait()
    pl.semaphore_wait(barrier, NZ - 1 + NP - 1 + NX - 1)
    far = sorted(range(1, NZ), key=lambda d: -min(d, NZ - d))
    for d in far:
        zt = zplus(d)
        remote(
            normed.at[:, pl.ds(pl.multiple_of(zt * kblock, kblock), kblock)], slices.at[z],
            send.at[0], recv.at[0], {"ep_0": zt},
        ).start()
    for i in range(1, NP):
        remote(wq.at[yc], wq.at[yc], send.at[1], recv.at[1], pplus(i)[1]).start()
    ld_wk.wait()
    ld_wv.wait()
    for i in range(1, NP):
        remote(wkv.at[yc], wkv.at[yc], send.at[2], recv.at[2], pplus(i)[1]).start()
    slices[pl.ds(z, 1)] = normed[:, pl.ds(pl.multiple_of(z * kblock, kblock), kblock)][None]

    wait_bytes(slices.at[pl.ds(0, NZ - 1)], recv.at[0])
    wait_bytes(wq.at[pl.ds(0, NP - 1)], recv.at[1])
    lhs = slices[...].reshape(NZ * seqs, kblock)
    part_q[...] = dot(lhs, wq[...].reshape(kblock, 2 * HD)).astype(BF16).reshape(NZ, seqs, 2 * HD)
    for d in far:
        zt = zplus(d)
        remote(part_q.at[zt], got_q.at[z], send.at[3], recv.at[3], {"ep_0": zt}).start()
    got_q[pl.ds(z, 1)] = part_q[pl.ds(z, 1)]

    wait_bytes(wkv.at[pl.ds(0, NP - 1)], recv.at[2])
    part_kv[...] = dot(lhs, wkv[...].reshape(kblock, 2 * HD)).astype(BF16).reshape(NZ, seqs, 2 * HD)
    for d in far:
        zt = zplus(d)
        remote(part_kv.at[zt], got_kv.at[z], send.at[4], recv.at[4], {"ep_0": zt}).start()
    got_kv[pl.ds(z, 1)] = part_kv[pl.ds(z, 1)]

    rows, cols = QB * seqs, NE * RB
    ld_rt.wait()
    ld_rw.wait()
    route = jnp.concatenate([route_v[...]] * QB, axis=0)
    rweight = jnp.concatenate([rweight_v[...]] * QB, axis=0)
    col = iota((rows, cols), 1)
    row = iota((rows, cols), 0)
    col_e = col // RB
    hit = jnp.zeros((rows, cols), F32)
    weighted = jnp.zeros((rows, cols), F32)
    for k in range(topk):
        same = route[:, k : k + 1] == col_e
        hit = jnp.where(same, 1.0, hit)
        weighted = jnp.where(same, rweight[:, k : k + 1], weighted)
    r0, r1 = iota((rows, rows), 0), iota((rows, rows), 1)
    earlier = ((r0 // seqs == r1 // seqs) & (r1 < r0)).astype(F32).astype(BF16)
    before = dot(earlier, hit.astype(BF16))
    chosen = (row // seqs == lax.rem(col, QB)) & (
        before == (lax.rem(col, RB) // QB).astype(F32)
    )
    place = jnp.where(chosen, hit, 0.0).astype(BF16)
    weighted = jnp.where(chosen, weighted, 0.0)
    weight_hi = weighted.astype(BF16)
    weight_lo = (weighted - weight_hi.astype(F32)).astype(BF16)

    hrow = iota((2 * seqs, 1), 0)
    seq_of = lax.rem(hrow, seqs)
    length_col = jnp.zeros((2 * seqs, 1), jnp.int32)
    for s in range(seqs):
        length_col = jnp.where(seq_of == s, lengths[s], length_col)
    bias_col = jnp.where(hrow < seqs, stay_bias[0], stay_bias[1])

    wait_bytes(got_q.at[pl.ds(0, NZ - 1)], recv.at[3])
    query = jnp.sum(got_q[...].astype(F32), axis=0)
    query = jnp.concatenate([query[:, :HD], query[:, HD:]], axis=0).astype(BF16).astype(F32)
    twice = jnp.concatenate([query, query], axis=1)
    pair_row = lax.rem(iota((2 * seqs, 2 * HD), 0), seqs) - iota((2 * seqs, 2 * HD), 1) // HD
    total = None
    for p in range(npair):
        ld_k[p].wait()
        block = jnp.where(pair_row == 2 * p, twice, 0.0).astype(BF16)
        keys = jnp.concatenate([kc[2 * p], kc[2 * p + 1]], axis=1)
        term = dot(block, keys, ((1,), (1,)))
        total = term if total is None else total + term
    zs = total * (HD ** -0.5) + bias_col
    live = iota((2 * seqs, cache_len), 1) < length_col
    log_stay = jnp.where(live, -(jnp.maximum(zs, 0.0) + jnp.log1p(jnp.exp(-jnp.abs(zs)))), 0.0)
    hi = log_stay.astype(BF16)
    lo = (log_stay - hi.astype(F32)).astype(BF16)
    blk = min(256, cache_len)
    tri = (iota((blk, blk), 0) >= iota((blk, blk), 1)).astype(F32).astype(BF16)
    carry = jnp.zeros((2 * seqs, 1), F32)
    for b in reversed(range(cache_len // blk)):
        at = slice(b * blk, (b + 1) * blk)
        within = dot(hi[:, at], tri) + dot(lo[:, at], tri)
        stick = jnp.where(live[:, at], jnp.exp(zs[:, at] + within + carry), 0.0)
        sticks[:, at] = stick.astype(BF16)
        carry = carry + within[:, 0:1]
    weights = sticks[...]
    att = jnp.zeros((2 * seqs, HD), F32)
    for p in range(npair):
        ld_v[p].wait()
        values = jnp.concatenate([vc[2 * p], vc[2 * p + 1]], axis=1)
        mixed = dot(weights, values)
        att = att + jnp.where(seq_of == 2 * p, mixed[:, :HD], 0.0)
        att = att + jnp.where(seq_of == 2 * p + 1, mixed[:, HD:], 0.0)
    att = att.astype(BF16)
    attended = jnp.concatenate([att[:seqs], att[seqs:]], axis=1)

    ld_ow.wait()
    hp_full = dot(attended, ow[...]).astype(BF16)
    for q in range(NX):
        hp[q] = hp_full[:, q * quarter : (q + 1) * quarter]
    xfar = sorted(range(1, NX), key=lambda d: -min(d, NX - d))
    for d in xfar:
        xt = xplus(d)
        remote(hp.at[xt], hr.at[x], send.at[5], recv.at[5], {"tp": xt}).start()
    hr[pl.ds(x, 1)] = hp[pl.ds(x, 1)]
    own_tok = tok[:, pl.ds(pl.multiple_of(x * quarter, quarter), quarter)].astype(F32)
    wait_bytes(hr.at[pl.ds(0, NX - 1)], recv.at[5])
    residual = (own_tok + jnp.sum(hr[...].astype(F32), axis=0)).astype(BF16)

    stacked = jnp.concatenate([residual[:, q * HD : (q + 1) * HD] for q in range(QB)], axis=0)
    outgoing = dot(place, stacked, ((0,), (0,)))
    sb[...] = outgoing.reshape(NE, RB, HD).astype(BF16)
    for k in sorted(range(NZ), key=lambda d: -min(d, NZ - d)):
        zt = zplus(NZ - k)

        def send_one(i, carry, k=k, zt=zt):
            j, dev = pplus(i)
            remote(
                sb.at[zt * NP + j], xg.at[x, me], send.at[6], chunk_recv.at[k], {"ep_0": zt, **dev}
            ).start()
            return carry

        lax.fori_loop(0 if k else 1, NP, send_one, 0)
    xg[x, pl.ds(me, 1)] = sb[pl.ds(me, 1)]

    order = sorted(range(NZ), key=lambda d: (min(d, NZ - d), d))
    groups = [tuple(order[g : g + 2]) for g in range(0, NZ, 2)]
    for g, ks in enumerate(groups):
        for k in ks:
            zc = pl.multiple_of(zplus(k) * NP, NP)
            wait_bytes(xg.at[0, pl.ds(0, NP if k else NP - 1)], chunk_recv.at[k])
            for d in xfar:
                remote(
                    xg.at[x, pl.ds(zc, NP)], xg.at[x, pl.ds(zc, NP)],
                    send.at[7], group_recv.at[g], {"tp": xplus(d)},
                ).start()

    slots = 2 * NP * CAP
    pr = iota((QB * slots, QB * slots), 0)
    pc = iota((QB * slots, QB * slots), 1)
    to_q = ((lax.rem(pc, QB) == pr // slots) & (pc // QB == lax.rem(pr, slots))).astype(F32).astype(BF16)
    from_q = ((lax.rem(pr, QB) == pc // slots) & (pr // QB == lax.rem(pc, slots))).astype(F32).astype(BF16)
    ld_gf.wait()
    gain = gain_f[...]

    def experts(g):
        ks = groups[g]
        wait_bytes(xg.at[0, pl.ds(0, (NX - 1) * 2 * NP)], group_recv.at[g])
        blocks = []
        for q in range(NX):
            two = [
                xg[q, pl.ds(pl.multiple_of(zplus(k) * NP, NP), NP)].astype(F32).reshape(NP * RB, HD)
                for k in ks
            ]
            blocks.append(jnp.concatenate(two, axis=0))
        raw = jnp.concatenate(blocks, axis=1).astype(BF16)
        ordered = dot(to_q, raw)
        res = jnp.concatenate(
            [
                ordered[q * slots : (q + 1) * slots, a * HD : (a + 1) * HD]
                for a in range(NX)
                for q in range(QB)
            ],
            axis=1,
        )
        ffn_in = rms_scale(res, gain).astype(BF16)
        if g == 0:
            ld_gw.wait()
            ld_uw.wait()
            ld_dw.wait()
        gate_pre = dot(ffn_in, gw[...])
        upward = dot(ffn_in, uw[...])
        capped = jnp.minimum(gate_pre, clamp_limit)
        upward = jnp.clip(upward, -clamp_limit, clamp_limit)
        units = (capped * jax.nn.sigmoid(gate_alpha * capped) * (upward + 1.0)).astype(BF16)
        down = dot(units, dw[...]).astype(BF16)
        for q in range(NX):
            epart[g, q] = down[:, q * quarter : (q + 1) * quarter]
        for d in xfar:
            xt = xplus(d)
            remote(epart.at[g, xt], egot.at[g, x], send.at[8], group_got.at[g], {"tp": xt}).start()
        egot[g, pl.ds(x, 1)] = epart[g, pl.ds(x, 1)]

    def give_back(g):
        wait_bytes(egot.at[g, pl.ds(0, NX - 1)], group_got.at[g])
        summed = jnp.sum(egot[g].astype(F32), axis=0).astype(BF16)
        stack = jnp.concatenate([summed[:, q * HD : (q + 1) * HD] for q in range(QB)], axis=0)
        back = dot(from_q, stack).reshape(2 * NP, RB, HD).astype(BF16)
        for n, k in enumerate(groups[g]):
            zc = zplus(k)
            rb[pl.ds(pl.multiple_of(zc * NP, NP), NP)] = back[n * NP : (n + 1) * NP]
        for k in groups[g]:
            zc = zplus(k)

            def send_one(i, carry, zc=zc):
                j, dev = pplus(i)
                remote(
                    rb.at[zc * NP + j], rt.at[me], send.at[9], recv.at[9], {"ep_0": zc, **dev}
                ).start()
                return carry

            lax.fori_loop(0 if k else 1, NP, send_one, 0)
            if k == 0:
                rt[pl.ds(me, 1)] = rb[pl.ds(me, 1)]

    G = len(groups)
    experts(0)
    for g in range(1, G):
        experts(g)
        give_back(g - 1)
    give_back(G - 1)

    wait_bytes(got_kv.at[pl.ds(0, NZ - 1)], recv.at[4])
    kv = jnp.sum(got_kv[...].astype(F32), axis=0).astype(BF16)
    new_keys[...] = kv[:, :HD]
    new_values[...] = kv[:, HD:]

    wait_bytes(slices.at[pl.ds(0, NZ - 1)], send.at[0])
    wait_bytes(wq.at[pl.ds(0, NP - 1)], send.at[1])
    wait_bytes(wkv.at[pl.ds(0, NP - 1)], send.at[2])
    wait_bytes(got_q.at[pl.ds(0, NZ - 1)], send.at[3])
    wait_bytes(got_kv.at[pl.ds(0, NZ - 1)], send.at[4])
    wait_bytes(hr.at[pl.ds(0, NX - 1)], send.at[5])
    wait_bytes(xg.at[0, pl.ds(0, NE - 1)], send.at[6])
    wait_bytes(xg.at[pl.ds(0, NX - 1)], send.at[7])
    wait_bytes(egot.at[pl.ds(0, G * (NX - 1) // NX)], send.at[8])

    wait_bytes(rt.at[pl.ds(0, NE - 1)], recv.at[9])
    back = rt[...].astype(F32).reshape(NE * RB, HD).astype(BF16)
    routed = dot(weight_hi, back) + dot(weight_lo, back)
    res_f = residual.astype(F32)
    for q in range(QB):
        at = slice(q * HD, (q + 1) * HD)
        layer_out[:, at] = (res_f[:, at] + routed[q * seqs : (q + 1) * seqs]).astype(BF16)
    wait_bytes(rt.at[pl.ds(0, NE - 1)], send.at[9])


def body(
    tokens, key_cache, value_cache, lengths, attn_gain, query_weight, key_weight, value_weight,
    stay_bias, out_weight, ffn_gain, gate_weight, up_weight, down_weight, routes, route_weight,
):
    sizes = tuple(lax.axis_size(a) for a in AXES)
    NZ, NY, NC, NX = sizes
    NP, NE = NY * NC, NZ * NY * NC
    seqs, width = tokens.shape
    cache_len = key_cache.shape[1]
    quarter = width // NX
    kblock = width // NZ
    QB = quarter // HD
    RB = CAP * QB
    hidden = gate_weight.shape[2]
    G = NZ // 2
    slots = 2 * NP * CAP
    vm = pltpu.VMEM
    scratch = [
        vm((seqs, width), BF16), vm((1, width), F32), vm((1, width), F32),
        vm(routes.shape, jnp.int32), vm(route_weight.shape, F32),
        vm(key_cache.shape, BF16), vm(value_cache.shape, BF16),
        vm(out_weight.shape, BF16), vm((width, hidden), BF16), vm((width, hidden), BF16),
        vm((hidden, width), BF16),
        vm((seqs, width), BF16),
        vm((NZ, seqs, kblock), BF16),
        vm((NP, kblock // NP, 2 * HD), BF16), vm((NP, kblock // NP, 2 * HD), BF16),
        vm((NZ, seqs, 2 * HD), BF16), vm((NZ, seqs, 2 * HD), BF16),
        vm((NZ, seqs, 2 * HD), BF16), vm((NZ, seqs, 2 * HD), BF16),
        vm((2 * seqs, cache_len), BF16),
        vm((NX, seqs, quarter), BF16), vm((NX, seqs, quarter), BF16),
        vm((NE, RB, HD), BF16), vm((NX, NE, RB, HD), BF16),
        vm((G, NX, slots, quarter), BF16), vm((G, NX, slots, quarter), BF16),
        vm((NE, RB, HD), BF16), vm((NE, RB, HD), BF16),
        pltpu.SemaphoreType.DMA((8,)), pltpu.SemaphoreType.DMA((2, seqs // 2)),
        pltpu.SemaphoreType.DMA((4,)),
        pltpu.SemaphoreType.DMA((10,)), pltpu.SemaphoreType.DMA((10,)),
        pltpu.SemaphoreType.DMA((NZ,)), pltpu.SemaphoreType.DMA((G,)), pltpu.SemaphoreType.DMA((G,)),
    ]
    hbm = pl.BlockSpec(memory_space=pl.ANY)
    smem = pl.BlockSpec(memory_space=pltpu.SMEM)
    in_specs = [hbm] * 16
    in_specs[3] = smem
    in_specs[8] = smem
    out = [
        jax.ShapeDtypeStruct((seqs, quarter), BF16),
        jax.ShapeDtypeStruct((seqs, HD), BF16),
        jax.ShapeDtypeStruct((seqs, HD), BF16),
    ]
    return tuple(pl.pallas_call(
        functools.partial(layer_kernel, sizes),
        out_shape=out,
        in_specs=in_specs,
        out_specs=[pl.BlockSpec(memory_space=pltpu.VMEM)] * 3,
        scratch_shapes=scratch,
        compiler_params=pltpu.CompilerParams(
            collective_id=0, has_side_effects=True, vmem_limit_bytes=60 * 1024 * 1024
        ),
    )(
        tokens, key_cache, value_cache, lengths, attn_gain.reshape(1, width), query_weight,
        key_weight, value_weight, stay_bias, out_weight, ffn_gain.reshape(1, width), gate_weight,
        up_weight, down_weight, routes, route_weight,
    ))


def solution(mesh):
    finer = Mesh(mesh.devices.reshape(8, 4, 2, mesh.shape["tp"]), AXES)
    placed = (
        P(EP, None), P(EP, None, "tp"), P(EP, None, "tp"), P(EP), P(), P(EP, "tp"), P(EP, "tp"),
        P(EP, "tp"), P("tp"), P("tp", None), P(), P(EP, None, "tp"), P(EP, None, "tp"),
        P(EP, "tp", None), P(EP, None), P(EP, None),
    )
    return jax.shard_map(
        body, mesh=finer, in_specs=placed,
        out_specs=(P(EP, "tp"), P(EP, "tp"), P(EP, "tp")), check_vma=False,
    )
```

```python
import functools
import math

import jax
import jax.numpy as jnp
from jax import lax
from jax.experimental import pallas as pl
from jax.experimental.pallas import tpu as pltpu
from jax.sharding import Mesh
from jax.sharding import PartitionSpec as P

AXES = ("ep_0", "ep_1", "ep_2", "tp")
EP = AXES[:3]
MESH = pl.DeviceIdType.MESH
F32 = jnp.float32
BF16 = jnp.bfloat16
HD = 128
CAP = 2
eps_norm = 1e-05
clamp_limit = 7.0
gate_alpha = 1.702


def dot(a, b, dims=((1,), (0,))):
    return lax.dot_general(a, b, (dims, ((), ())), preferred_element_type=F32)


def rms_scale(values, gain):
    scale = lax.rsqrt(jnp.mean(values * values, axis=-1, keepdims=True) + eps_norm)
    return values * scale * gain


def iota(shape, dim):
    return lax.broadcasted_iota(jnp.int32, shape, dim)


def groups_of(near):
    return [tuple(near[3:5]), tuple(near[5:]), tuple(near[:3])]


def layer_kernel(
    sizes,
    tokens, key_cache, value_cache, lengths, attn_gain, query_weight, key_weight, value_weight,
    stay_bias, out_weight, ffn_gain, gate_weight, up_weight, down_weight, routes, route_weight,
    layer_out, new_keys, new_values,
    tok, gain_a, gain_f, route_v, rweight_v, kc, vc, ow, gw, uw, dw,
    normed, slices, wq, wkv, part_q, part_kv, got_q, got_kv,
    sticks, hp, hr, sb, xg, epart, egot, rb, rt,
    loc, kv_sem, exp_sem, send, recv, chunk_recv, group_recv, group_got,
):
    NZ, NY, NC, NX = sizes
    NP = NY * NC
    NE = NZ * NP
    z, y, c, x = (lax.axis_index(a) for a in AXES)
    yc = y * NC + c
    me = z * NP + yc
    seqs, width = tok.shape
    kblock = width // NZ
    quarter = width // NX
    QB = quarter // HD
    cache_len = kc.shape[1]
    RB = CAP * QB
    topk = route_v.shape[0]

    def zplus(d):
        return lax.rem(z + d, NZ)

    plane = []
    for i in range(NP):
        j = lax.rem(yc + i, NP)
        plane.append((j, {"ep_1": j // NC, "ep_2": lax.rem(j, NC)}))

    def pplus(i):
        return plane[i]

    def xplus(d):
        return lax.rem(x + d, NX)

    barrier = pltpu.get_barrier_semaphore()
    for d in range(1, NZ):
        pl.semaphore_signal(barrier, inc=1, device_id={"ep_0": zplus(d)}, device_id_type=MESH)
    for i in range(1, NP):
        pl.semaphore_signal(barrier, inc=1, device_id=pplus(i)[1], device_id_type=MESH)
    for d in range(1, NX):
        pl.semaphore_signal(barrier, inc=1, device_id={"tp": xplus(d)}, device_id_type=MESH)

    def load(src, dst, sem):
        copy = pltpu.make_async_copy(src, dst, sem)
        copy.start()
        return copy

    ld_tok = load(tokens, tok, loc.at[0])
    ld_ga = load(attn_gain, gain_a, loc.at[1])
    ld_wq = load(query_weight, wq.at[yc], loc.at[2])
    ld_wk = load(key_weight, wkv.at[yc, :, pl.ds(0, HD)], loc.at[3])
    ld_wv = load(value_weight, wkv.at[yc, :, pl.ds(HD, HD)], loc.at[4])
    ld_rt = load(routes, route_v, loc.at[5])
    ld_rw = load(route_weight, rweight_v, loc.at[6])
    ld_gf = load(ffn_gain, gain_f, loc.at[7])
    npair = seqs // 2
    ld_k = [load(key_cache.at[pl.ds(2 * p, 2)], kc.at[pl.ds(2 * p, 2)], kv_sem.at[0, p]) for p in range(npair)]
    ld_v = [load(value_cache.at[pl.ds(2 * p, 2)], vc.at[pl.ds(2 * p, 2)], kv_sem.at[1, p]) for p in range(npair)]
    ld_ow = load(out_weight, ow, exp_sem.at[0])
    ld_gw = load(gate_weight.at[0], gw, exp_sem.at[1])
    ld_uw = load(up_weight.at[0], uw, exp_sem.at[2])
    ld_dw = load(down_weight.at[0], dw, exp_sem.at[3])

    def remote(src, dst, s, r, device):
        return pltpu.make_async_remote_copy(
            src_ref=src, dst_ref=dst, send_sem=s, recv_sem=r, device_id=device, device_id_type=MESH
        )

    def wait_bytes(ref, sem):
        pltpu.make_async_copy(ref, ref, sem).wait()

    ld_tok.wait()
    ld_ga.wait()
    normed[...] = rms_scale(tok[...].astype(F32), gain_a[...]).astype(BF16)
    ld_wq.wait()
    pl.semaphore_wait(barrier, NZ - 1 + NP - 1 + NX - 1)
    far = sorted(range(1, NZ), key=lambda d: -min(d, NZ - d))
    for d in far:
        zt = zplus(d)
        remote(
            normed.at[:, pl.ds(pl.multiple_of(zt * kblock, kblock), kblock)], slices.at[z],
            send.at[0], recv.at[0], {"ep_0": zt},
        ).start()
    for i in range(1, NP):
        remote(wq.at[yc], wq.at[yc], send.at[1], recv.at[1], pplus(i)[1]).start()
    ld_wk.wait()
    ld_wv.wait()
    for i in range(1, NP):
        remote(wkv.at[yc], wkv.at[yc], send.at[2], recv.at[2], pplus(i)[1]).start()
    slices[pl.ds(z, 1)] = normed[:, pl.ds(pl.multiple_of(z * kblock, kblock), kblock)][None]

    wait_bytes(slices.at[pl.ds(0, NZ - 1)], recv.at[0])
    wait_bytes(wq.at[pl.ds(0, NP - 1)], recv.at[1])
    lhs = slices[...].reshape(NZ * seqs, kblock)
    part_q[...] = dot(lhs, wq[...].reshape(kblock, 2 * HD)).astype(BF16).reshape(NZ, seqs, 2 * HD)
    for d in far:
        zt = zplus(d)
        remote(part_q.at[zt], got_q.at[z], send.at[3], recv.at[3], {"ep_0": zt}).start()
    got_q[pl.ds(z, 1)] = part_q[pl.ds(z, 1)]

    wait_bytes(wkv.at[pl.ds(0, NP - 1)], recv.at[2])
    part_kv[...] = dot(lhs, wkv[...].reshape(kblock, 2 * HD)).astype(BF16).reshape(NZ, seqs, 2 * HD)
    for d in far:
        zt = zplus(d)
        remote(part_kv.at[zt], got_kv.at[z], send.at[4], recv.at[4], {"ep_0": zt}).start()
    got_kv[pl.ds(z, 1)] = part_kv[pl.ds(z, 1)]

    rows, cols = QB * seqs, NE * RB
    ld_rt.wait()
    ld_rw.wait()
    col = iota((rows, cols), 1)
    row = iota((rows, cols), 0)
    col_e = (col // RB).astype(F32)
    diag = lax.rem(iota((rows, seqs), 0), seqs) == iota((rows, seqs), 1)
    hit = jnp.zeros((rows, cols), F32)
    weighted = jnp.zeros((rows, cols), F32)

    def column(line):
        return jnp.sum(jnp.where(diag, line, 0.0), axis=1, keepdims=True)

    for k in range(topk):
        same = column(route_v[k : k + 1, :].astype(F32)) == col_e
        hit = jnp.where(same, 1.0, hit)
        weighted = jnp.where(same, column(rweight_v[k : k + 1, :]), weighted)
    r0, r1 = iota((rows, rows), 0), iota((rows, rows), 1)
    earlier = ((r0 // seqs == r1 // seqs) & (r1 < r0)).astype(F32).astype(BF16)
    before = dot(earlier, hit.astype(BF16))
    chosen = (row // seqs == lax.rem(col, QB)) & (
        before == (lax.rem(col, RB) // QB).astype(F32)
    )
    place = jnp.where(chosen, hit, 0.0).astype(BF16)
    weighted = jnp.where(chosen, weighted, 0.0)
    weight_hi = weighted.astype(BF16)
    weight_lo = (weighted - weight_hi.astype(F32)).astype(BF16)

    hrow = iota((2 * seqs, 1), 0)
    seq_of = lax.rem(hrow, seqs)
    length_col = jnp.zeros((2 * seqs, 1), jnp.int32)
    for s in range(seqs):
        length_col = jnp.where(seq_of == s, lengths[s], length_col)
    bias_col = jnp.where(hrow < seqs, stay_bias[0], stay_bias[1])

    wait_bytes(got_q.at[pl.ds(0, NZ - 1)], recv.at[3])
    query = jnp.sum(got_q[...].astype(F32), axis=0)
    query = jnp.concatenate([query[:, :HD], query[:, HD:]], axis=0).astype(BF16).astype(F32)
    twice = jnp.concatenate([query, query], axis=1)
    pair_row = lax.rem(iota((2 * seqs, 2 * HD), 0), seqs) - iota((2 * seqs, 2 * HD), 1) // HD
    total = None
    for p in range(npair):
        ld_k[p].wait()
        block = jnp.where(pair_row == 2 * p, twice, 0.0).astype(BF16)
        keys = jnp.concatenate([kc[2 * p], kc[2 * p + 1]], axis=1)
        term = dot(block, keys, ((1,), (1,)))
        total = term if total is None else total + term
    zs = total * (HD ** -0.5) + bias_col
    live = iota((2 * seqs, cache_len), 1) < length_col
    log_stay = jnp.where(live, -(jnp.maximum(zs, 0.0) + jnp.log1p(jnp.exp(-jnp.abs(zs)))), 0.0)
    hi = log_stay.astype(BF16)
    lo = (log_stay - hi.astype(F32)).astype(BF16)
    blk = min(256, cache_len)
    tri = (iota((blk, blk), 0) >= iota((blk, blk), 1)).astype(F32).astype(BF16)
    carry = jnp.zeros((2 * seqs, 1), F32)
    for b in reversed(range(cache_len // blk)):
        at = slice(b * blk, (b + 1) * blk)
        within = dot(hi[:, at], tri) + dot(lo[:, at], tri)
        stick = jnp.where(live[:, at], jnp.exp(zs[:, at] + within + carry), 0.0)
        sticks[:, at] = stick.astype(BF16)
        carry = carry + within[:, 0:1]
    weights = sticks[...]
    att = jnp.zeros((2 * seqs, HD), F32)
    for p in range(0, npair, 2):
        ld_v[p].wait()
        ld_v[p + 1].wait()
        four = range(2 * p, 2 * p + 4)
        mixed = dot(weights, jnp.concatenate([vc[n] for n in four], axis=1))
        for i, n in enumerate(four):
            att = att + jnp.where(seq_of == n, mixed[:, i * HD : (i + 1) * HD], 0.0)
    att = att.astype(BF16)
    attended = jnp.concatenate([att[:seqs], att[seqs:]], axis=1)

    near = sorted(range(NZ), key=lambda d: (min(d, NZ - d), d))
    groups = groups_of(near)
    ld_ow.wait()
    hp_full = dot(attended, ow[...]).astype(BF16)
    for q in range(NX):
        hp[q] = hp_full[:, q * quarter : (q + 1) * quarter]
    xfar = sorted(range(1, NX), key=lambda d: -min(d, NX - d))
    for d in xfar:
        xt = xplus(d)
        remote(hp.at[xt], hr.at[x], send.at[5], recv.at[5], {"tp": xt}).start()
    hr[pl.ds(x, 1)] = hp[pl.ds(x, 1)]
    own_tok = tok[:, pl.ds(pl.multiple_of(x * quarter, quarter), quarter)].astype(F32)
    wait_bytes(hr.at[pl.ds(0, NX - 1)], recv.at[5])
    residual = (own_tok + jnp.sum(hr[...].astype(F32), axis=0)).astype(BF16)

    stacked = jnp.concatenate([residual[:, q * HD : (q + 1) * HD] for q in range(QB)], axis=0)
    outgoing = dot(place, stacked, ((0,), (0,)))
    sb[...] = outgoing.reshape(NE, RB, HD).astype(BF16)
    for k in near:
        zt = zplus(NZ - k)
        for i in range(0 if k else 1, NP):
            j, dev = pplus(i)
            remote(
                sb.at[zt * NP + j], xg.at[x, me], send.at[6], chunk_recv.at[k], {"ep_0": zt, **dev}
            ).start()
    xg[x, pl.ds(me, 1)] = sb[pl.ds(me, 1)]

    for g, ks in enumerate(groups):
        for k in ks:
            zc = pl.multiple_of(zplus(k) * NP, NP)
            wait_bytes(xg.at[0, pl.ds(0, NP if k else NP - 1)], chunk_recv.at[k])
            for d in xfar:
                remote(
                    xg.at[x, pl.ds(zc, NP)], xg.at[x, pl.ds(zc, NP)],
                    send.at[7], group_recv.at[g], {"tp": xplus(d)},
                ).start()

    slots = NP * CAP
    pr = iota((QB * slots, QB * slots), 0)
    pc = iota((QB * slots, QB * slots), 1)
    to_q = ((lax.rem(pc, QB) == pr // slots) & (pc // QB == lax.rem(pr, slots))).astype(F32).astype(BF16)
    from_q = ((lax.rem(pr, QB) == pc // slots) & (pr // QB == lax.rem(pc, slots))).astype(F32).astype(BF16)
    ld_gf.wait()
    gain = gain_f[...]
    starts = [slots * sum(len(ks) for ks in groups[:g]) for g in range(len(groups))]

    def experts(g):
        ks = groups[g]
        at = pl.ds(starts[g], slots * len(ks))
        wait_bytes(xg.at[pl.ds(0, NX - 1), pl.ds(0, len(ks) * NP)], group_recv.at[g])
        raw = jnp.concatenate(
            [
                xg[a, pl.ds(pl.multiple_of(zplus(k) * NP, NP), NP)].astype(F32).reshape(NP * RB, HD)
                for k in ks
                for a in range(NX)
            ],
            axis=1,
        ).astype(BF16)
        ordered = dot(to_q, raw)
        res = jnp.concatenate(
            [
                jnp.concatenate(
                    [
                        ordered[q * slots : (q + 1) * slots, (n * NX + a) * HD : (n * NX + a + 1) * HD]
                        for a in range(NX)
                        for q in range(QB)
                    ],
                    axis=1,
                )
                for n in range(len(ks))
            ],
            axis=0,
        )
        ffn_in = rms_scale(res, gain).astype(BF16)
        if g == 0:
            ld_gw.wait()
            ld_uw.wait()
            ld_dw.wait()
        gate_pre = dot(ffn_in, gw[...])
        upward = dot(ffn_in, uw[...])
        capped = jnp.minimum(gate_pre, clamp_limit)
        upward = jnp.clip(upward, -clamp_limit, clamp_limit)
        units = (capped * jax.nn.sigmoid(gate_alpha * capped) * (upward + 1.0)).astype(BF16)
        down = dot(units, dw[...]).astype(BF16)
        for q in range(NX):
            epart[q, at] = down[:, q * quarter : (q + 1) * quarter]
        for d in xfar:
            xt = xplus(d)
            remote(epart.at[xt, at], egot.at[x, at], send.at[8], group_got.at[g], {"tp": xt}).start()
        egot[x, at] = epart[x, at]

    def give_back(g):
        ks = groups[g]
        at = pl.ds(starts[g], slots * len(ks))
        wait_bytes(egot.at[pl.ds(0, NX - 1), at], group_got.at[g])
        summed = jnp.sum(egot[:, at].astype(F32), axis=0).astype(BF16)
        stack = jnp.concatenate(
            [
                jnp.concatenate(
                    [summed[n * slots : (n + 1) * slots, q * HD : (q + 1) * HD] for q in range(QB)],
                    axis=0,
                )
                for n in range(len(ks))
            ],
            axis=1,
        )
        back = dot(from_q, stack)
        for n, k in enumerate(ks):
            block = back[:, n * HD : (n + 1) * HD].reshape(NP, RB, HD).astype(BF16)
            rb[pl.ds(pl.multiple_of(zplus(k) * NP, NP), NP)] = block
        for k in ks:
            zc = zplus(k)
            for i in range(0 if k else 1, NP):
                j, dev = pplus(i)
                remote(
                    rb.at[zc * NP + j], rt.at[me], send.at[9], recv.at[9], {"ep_0": zc, **dev}
                ).start()
            if k == 0:
                rt[pl.ds(me, 1)] = rb[pl.ds(me, 1)]

    G = len(groups)
    experts(0)
    for g in range(1, G):
        experts(g)
        give_back(g - 1)
    give_back(G - 1)

    wait_bytes(got_kv.at[pl.ds(0, NZ - 1)], recv.at[4])
    kv = jnp.sum(got_kv[...].astype(F32), axis=0).astype(BF16)
    new_keys[...] = kv[:, :HD]
    new_values[...] = kv[:, HD:]

    wait_bytes(slices.at[pl.ds(0, NZ - 1)], send.at[0])
    wait_bytes(wq.at[pl.ds(0, NP - 1)], send.at[1])
    wait_bytes(wkv.at[pl.ds(0, NP - 1)], send.at[2])
    wait_bytes(got_q.at[pl.ds(0, NZ - 1)], send.at[3])
    wait_bytes(got_kv.at[pl.ds(0, NZ - 1)], send.at[4])
    wait_bytes(hr.at[pl.ds(0, NX - 1)], send.at[5])
    wait_bytes(xg.at[0, pl.ds(0, NE - 1)], send.at[6])
    wait_bytes(xg.at[pl.ds(0, NX - 1)], send.at[7])
    wait_bytes(egot.at[pl.ds(0, NX - 1)], send.at[8])

    wait_bytes(rt.at[pl.ds(0, NE - 1)], recv.at[9])
    back = rt[...].astype(F32).reshape(NE * RB, HD).astype(BF16)
    routed = dot(weight_hi, back) + dot(weight_lo, back)
    res_f = residual.astype(F32)
    for q in range(QB):
        at = slice(q * HD, (q + 1) * HD)
        layer_out[:, at] = (res_f[:, at] + routed[q * seqs : (q + 1) * seqs]).astype(BF16)
    wait_bytes(rt.at[pl.ds(0, NE - 1)], send.at[9])


def tail_kernel(layer_in, keys_in, values_in, layer_out, new_keys, new_values):
    layer_out[...] = layer_in[...]
    new_keys[...] = keys_in[...]
    new_values[...] = values_in[...]


def body(
    tokens, key_cache, value_cache, lengths, attn_gain, query_weight, key_weight, value_weight,
    stay_bias, out_weight, ffn_gain, gate_weight, up_weight, down_weight, routes, route_weight,
):
    routes, route_weight = routes.T, route_weight.T
    sizes = tuple(lax.axis_size(a) for a in AXES)
    NZ, NY, NC, NX = sizes
    NP, NE = NY * NC, NZ * NY * NC
    seqs, width = tokens.shape
    cache_len = key_cache.shape[1]
    quarter = width // NX
    kblock = width // NZ
    QB = quarter // HD
    RB = CAP * QB
    hidden = gate_weight.shape[2]
    G = len(groups_of(list(range(NZ))))
    vm = pltpu.VMEM
    scratch = [
        vm((seqs, width), BF16), vm((1, width), F32), vm((1, width), F32),
        vm(routes.shape, jnp.int32), vm(route_weight.shape, F32),
        vm(key_cache.shape, BF16), vm(value_cache.shape, BF16),
        vm(out_weight.shape, BF16), vm((width, hidden), BF16), vm((width, hidden), BF16),
        vm((hidden, width), BF16),
        vm((seqs, width), BF16),
        vm((NZ, seqs, kblock), BF16),
        vm((NP, kblock // NP, 2 * HD), BF16), vm((NP, kblock // NP, 2 * HD), BF16),
        vm((NZ, seqs, 2 * HD), BF16), vm((NZ, seqs, 2 * HD), BF16),
        vm((NZ, seqs, 2 * HD), BF16), vm((NZ, seqs, 2 * HD), BF16),
        vm((2 * seqs, cache_len), BF16),
        vm((NX, seqs, quarter), BF16), vm((NX, seqs, quarter), BF16),
        vm((NE, RB, HD), BF16), vm((NX, NE, RB, HD), BF16),
        vm((NX, NE * CAP, quarter), BF16), vm((NX, NE * CAP, quarter), BF16),
        vm((NE, RB, HD), BF16), vm((NE, RB, HD), BF16),
        pltpu.SemaphoreType.DMA((8,)), pltpu.SemaphoreType.DMA((2, seqs // 2)),
        pltpu.SemaphoreType.DMA((4,)),
        pltpu.SemaphoreType.DMA((10,)), pltpu.SemaphoreType.DMA((10,)),
        pltpu.SemaphoreType.DMA((NZ,)), pltpu.SemaphoreType.DMA((G,)), pltpu.SemaphoreType.DMA((G,)),
    ]
    hbm = pl.BlockSpec(memory_space=pl.ANY)
    smem = pl.BlockSpec(memory_space=pltpu.SMEM)
    in_specs = [hbm] * 16
    in_specs[3] = smem
    in_specs[8] = smem
    out = [
        jax.ShapeDtypeStruct((seqs, quarter), BF16),
        jax.ShapeDtypeStruct((seqs, HD), BF16),
        jax.ShapeDtypeStruct((seqs, HD), BF16),
    ]
    parts = pl.pallas_call(
        functools.partial(layer_kernel, sizes),
        out_shape=out,
        in_specs=in_specs,
        out_specs=[pl.BlockSpec(memory_space=pltpu.VMEM)] * 3,
        scratch_shapes=scratch,
        compiler_params=pltpu.CompilerParams(
            collective_id=0, has_side_effects=True, vmem_limit_bytes=60 * 1024 * 1024
        ),
    )(
        tokens, key_cache, value_cache, lengths, attn_gain.reshape(1, width), query_weight,
        key_weight, value_weight, stay_bias, out_weight, ffn_gain.reshape(1, width), gate_weight,
        up_weight, down_weight, routes, route_weight,
    )
    vmem = pl.BlockSpec(memory_space=pltpu.VMEM)
    return tuple(pl.pallas_call(
        tail_kernel, out_shape=out, in_specs=[vmem] * 3, out_specs=[vmem] * 3,
    )(*parts))


def solution(mesh):
    finer = Mesh(mesh.devices.reshape(8, 4, 2, mesh.shape["tp"]), AXES)
    placed = (
        P(EP, None), P(EP, None, "tp"), P(EP, None, "tp"), P(EP), P(), P(EP, "tp"), P(EP, "tp"),
        P(EP, "tp"), P("tp"), P("tp", None), P(), P(EP, None, "tp"), P(EP, None, "tp"),
        P(EP, "tp", None), P(EP, None), P(EP, None),
    )
    return jax.shard_map(
        body, mesh=finer, in_specs=placed,
        out_specs=(P(EP, "tp"), P(EP, "tp"), P(EP, "tp")), check_vma=False,
    )
```

```python
import functools
import math

import jax
import jax.numpy as jnp
from jax import lax
from jax.experimental import pallas as pl
from jax.experimental.pallas import tpu as pltpu
from jax.sharding import Mesh
from jax.sharding import PartitionSpec as P

AXES = ("ep_0", "ep_1", "ep_2", "tp")
EP = AXES[:3]
MESH = pl.DeviceIdType.MESH
F32 = jnp.float32
BF16 = jnp.bfloat16
HD = 128
CAP = 2
eps_norm = 1e-05
clamp_limit = 7.0
gate_alpha = 1.702

def dot(a, b, dims=((1,), (0,))):
    return lax.dot_general(a, b, (dims, ((), ())), preferred_element_type=F32)

def rms_scale(values, gain):
    scale = lax.rsqrt(jnp.mean(values * values, axis=-1, keepdims=True) + eps_norm)
    return values * scale * gain

def iota(shape, dim):
    return lax.broadcasted_iota(jnp.int32, shape, dim)

DIRECT = 3

def groups_of(near):
    return [tuple(near[DIRECT:6]), tuple(near[6:])]

def layer_kernel(
    sizes,
    tokens, key_cache, value_cache, lengths_in, attn_gain, query_weight, key_weight, value_weight,
    bias_in, out_weight, ffn_gain, gate_weight, up_weight, down_weight, routes, route_weight,
    layer_out, new_keys, new_values,
    resx, sbn, xn, rbn, rtn, nps, npr, lengths, stay_bias, tok, gain_a, gain_f, route_v, rweight_v, kc, vc, ow, gw, uw, dw,
    normed, slices, wq, wkv, part_q, part_kv, got_q, got_kv,
    sticks, hp, hr, sb, xg, epart, egot, rb, rt,
    loc, kv_sem, exp_sem, send, recv, chunk_recv, group_recv, group_got,
):
    NZ, NY, NC, NX = sizes
    NP = NY * NC
    NE = NZ * NP
    z, y, c, x = (lax.axis_index(a) for a in AXES)
    yc = y * NC + c
    me = z * NP + yc
    seqs, width = tok.shape
    kblock = width // NZ
    quarter = width // NX
    QB = quarter // HD
    cache_len = kc.shape[1]
    RB = CAP * QB
    topk = route_v.shape[0]

    def zplus(d):
        return lax.rem(z + d, NZ)

    plane = []
    for i in range(NP):
        j = lax.rem(yc + i, NP)
        plane.append((j, {"ep_1": j // NC, "ep_2": lax.rem(j, NC)}))

    def pplus(i):
        return plane[i]

    def xplus(d):
        return lax.rem(x + d, NX)

    barrier = pltpu.get_barrier_semaphore()
    for d in range(1, NZ):
        pl.semaphore_signal(barrier, inc=1, device_id={"ep_0": zplus(d)}, device_id_type=MESH)
    for i in range(1, NP):
        pl.semaphore_signal(barrier, inc=1, device_id=pplus(i)[1], device_id_type=MESH)
    for d in range(1, NX):
        pl.semaphore_signal(barrier, inc=1, device_id={"tp": xplus(d)}, device_id_type=MESH)

    def load(src, dst, sem):
        copy = pltpu.make_async_copy(src, dst, sem)
        copy.start()
        return copy

    ld_tok = load(tokens, tok, loc.at[0])
    ld_ga = load(attn_gain, gain_a, loc.at[1])
    ld_wq = load(query_weight, wq.at[yc], loc.at[2])
    ld_wk = load(key_weight, wkv.at[yc, :, pl.ds(0, HD)], loc.at[3])
    ld_wv = load(value_weight, wkv.at[yc, :, pl.ds(HD, HD)], loc.at[4])
    ld_rt = load(routes, route_v, loc.at[5])
    ld_rw = load(route_weight, rweight_v, loc.at[6])
    ld_gf = load(ffn_gain, gain_f, loc.at[7])
    ld_len = load(lengths_in, lengths, loc.at[8])
    ld_bias = load(bias_in, stay_bias, loc.at[9])
    npair = seqs // 2
    ld_k = [load(key_cache.at[pl.ds(2 * p, 2)], kc.at[pl.ds(2 * p, 2)], kv_sem.at[0, p]) for p in range(npair)]
    ld_v = [load(value_cache.at[pl.ds(2 * p, 2)], vc.at[pl.ds(2 * p, 2)], kv_sem.at[1, p]) for p in range(npair)]
    ld_ow = load(out_weight, ow, exp_sem.at[0])
    ld_gw = load(gate_weight.at[0], gw, exp_sem.at[1])
    ld_uw = load(up_weight.at[0], uw, exp_sem.at[2])
    ld_dw = load(down_weight.at[0], dw, exp_sem.at[3])

    def remote(src, dst, s, r, device):
        return pltpu.make_async_remote_copy(
            src_ref=src, dst_ref=dst, send_sem=s, recv_sem=r, device_id=device, device_id_type=MESH
        )

    def wait_bytes(ref, sem):
        pltpu.make_async_copy(ref, ref, sem).wait()


    ld_tok.wait()
    ld_ga.wait()
    normed[...] = rms_scale(tok[...].astype(F32), gain_a[...]).astype(BF16)
    ld_wq.wait()

    pl.semaphore_wait(barrier, NZ - 1 + NP - 1 + NX - 1)

    far = sorted(range(1, NZ), key=lambda d: -min(d, NZ - d))
    for d in far:
        zt = zplus(d)
        remote(
            normed.at[:, pl.ds(pl.multiple_of(zt * kblock, kblock), kblock)], slices.at[z],
            send.at[0], recv.at[0], {"ep_0": zt},
        ).start()
    for i in range(1, NP):
        remote(wq.at[yc], wq.at[yc], send.at[1], recv.at[1], pplus(i)[1]).start()
    ld_wk.wait()
    ld_wv.wait()
    for i in range(1, NP):
        remote(wkv.at[yc], wkv.at[yc], send.at[2], recv.at[2], pplus(i)[1]).start()
    slices[pl.ds(z, 1)] = normed[:, pl.ds(pl.multiple_of(z * kblock, kblock), kblock)][None]

    rt[...] = jnp.zeros_like(rt)
    rtn[...] = jnp.zeros_like(rtn)

    wait_bytes(slices.at[pl.ds(0, NZ - 1)], recv.at[0])

    wait_bytes(wq.at[pl.ds(0, NP - 1)], recv.at[1])

    lhs = slices[...].reshape(NZ * seqs, kblock)
    part_q[...] = dot(lhs, wq[...].reshape(kblock, 2 * HD)).astype(BF16).reshape(NZ, seqs, 2 * HD)
    for d in far:
        zt = zplus(d)
        remote(part_q.at[zt], got_q.at[z], send.at[3], recv.at[3], {"ep_0": zt}).start()
    got_q[pl.ds(z, 1)] = part_q[pl.ds(z, 1)]

    rows, cols = QB * seqs, NE * RB
    ld_rt.wait()
    ld_rw.wait()
    col = iota((rows, cols), 1)
    row = iota((rows, cols), 0)
    col_e = (col // RB).astype(F32)
    diag = lax.rem(iota((rows, seqs), 0), seqs) == iota((rows, seqs), 1)
    hit = jnp.zeros((rows, cols), F32)
    weighted = jnp.zeros((rows, cols), F32)

    def column(line):
        return jnp.sum(jnp.where(diag, line, 0.0), axis=1, keepdims=True)

    for k in range(topk):
        same = column(route_v[k : k + 1, :].astype(F32)) == col_e
        hit = jnp.where(same, 1.0, hit)
        weighted = jnp.where(same, column(rweight_v[k : k + 1, :]), weighted)
    r0, r1 = iota((rows, rows), 0), iota((rows, rows), 1)
    earlier = ((r0 // seqs == r1 // seqs) & (r1 < r0)).astype(F32).astype(BF16)
    before = dot(earlier, hit.astype(BF16))
    chosen = (row // seqs == lax.rem(col, QB)) & (
        before == (lax.rem(col, RB) // QB).astype(F32)
    )
    place = jnp.where(chosen, hit, 0.0).astype(BF16)
    weighted = jnp.where(chosen, weighted, 0.0)
    weight_hi = weighted.astype(BF16)
    weight_lo = (weighted - weight_hi.astype(F32)).astype(BF16)

    ld_len.wait()
    ld_bias.wait()
    hrow = iota((2 * seqs, 1), 0)
    seq_of = lax.rem(hrow, seqs)
    length_col = jnp.zeros((2 * seqs, 1), jnp.int32)
    for s in range(seqs):
        length_col = jnp.where(seq_of == s, lengths[s], length_col)
    bias_col = jnp.where(hrow < seqs, stay_bias[0], stay_bias[1])

    wait_bytes(got_q.at[pl.ds(0, NZ - 1)], recv.at[3])

    query = jnp.sum(got_q[...].astype(F32), axis=0)
    query = jnp.concatenate([query[:, :HD], query[:, HD:]], axis=0).astype(BF16).astype(F32)
    for p in range(npair):
        ld_k[p].wait()
    block = jnp.concatenate([jnp.where(seq_of == n, query, 0.0) for n in range(seqs)], axis=1)
    keys = jnp.concatenate([kc[n] for n in range(seqs)], axis=1)
    total = dot(block.astype(BF16), keys, ((1,), (1,)))

    zs = total * (HD ** -0.5) + bias_col
    live = iota((2 * seqs, cache_len), 1) < length_col
    log_stay = jnp.where(live, -(jnp.maximum(zs, 0.0) + jnp.log1p(jnp.exp(-jnp.abs(zs)))), 0.0)
    hi = log_stay.astype(BF16)
    lo = (log_stay - hi.astype(F32)).astype(BF16)
    blk = min(256, cache_len)
    tri = (iota((blk, blk), 0) >= iota((blk, blk), 1)).astype(F32).astype(BF16)
    carry = jnp.zeros((2 * seqs, 1), F32)
    for b in reversed(range(cache_len // blk)):
        at = slice(b * blk, (b + 1) * blk)
        within = dot(hi[:, at], tri) + dot(lo[:, at], tri)
        stick = jnp.where(live[:, at], jnp.exp(zs[:, at] + within + carry), 0.0)
        sticks[:, at] = stick.astype(BF16)
        carry = carry + within[:, 0:1]

    weights = sticks[...]
    att = jnp.zeros((2 * seqs, HD), F32)
    for p in range(npair):
        ld_v[p].wait()
    mixed = dot(weights, jnp.concatenate([vc[n] for n in range(seqs)], axis=1))
    for n in range(seqs):
        att = att + jnp.where(seq_of == n, mixed[:, n * HD : (n + 1) * HD], 0.0)
    att = att.astype(BF16)
    attended = jnp.concatenate([att[:seqs], att[seqs:]], axis=1)

    near = sorted(range(NZ), key=lambda d: (min(d, NZ - d), d))
    groups = groups_of(near)
    direct, far_ks = near[:DIRECT], [k for ks in groups for k in ks]

    ld_ow.wait()
    xfar = sorted(range(1, NX), key=lambda d: -min(d, NX - d))

    hp_full = dot(attended, ow[...]).astype(BF16)
    for q in range(NX):
        hp[q] = hp_full[:, q * quarter : (q + 1) * quarter]

    for d in xfar:
        xt = xplus(d)
        remote(hp.at[xt], hr.at[x], send.at[5], recv.at[5], {"tp": xt}).start()
    hr[pl.ds(x, 1)] = hp[pl.ds(x, 1)]
    own_tok = tok[:, pl.ds(pl.multiple_of(x * quarter, quarter), quarter)].astype(F32)

    wait_bytes(wkv.at[pl.ds(0, NP - 1)], recv.at[2])

    part_kv[...] = dot(lhs, wkv[...].reshape(kblock, 2 * HD)).astype(BF16).reshape(NZ, seqs, 2 * HD)
    for d in far:
        zt = zplus(d)
        remote(part_kv.at[zt], got_kv.at[z], send.at[4], recv.at[4], {"ep_0": zt}).start()
    got_kv[pl.ds(z, 1)] = part_kv[pl.ds(z, 1)]

    wait_bytes(hr.at[pl.ds(0, NX - 1)], recv.at[5])

    residual = (own_tok + jnp.sum(hr[...].astype(F32), axis=0)).astype(BF16)

    resx[pl.ds(x, 1)] = residual[None]
    stacked = jnp.concatenate([residual[:, q * HD : (q + 1) * HD] for q in range(QB)], axis=0)
    outgoing = dot(place, stacked, ((0,), (0,)))
    sb[...] = outgoing.reshape(NE, RB, HD).astype(BF16)

    for k in far_ks:
        zt = zplus(NZ - k)
        for i in range(NP):
            j, dev = pplus(i)
            remote(
                sb.at[zt * NP + j], xg.at[x, me], send.at[6], chunk_recv.at[k], {"ep_0": zt, **dev}
            ).start()
    for d in xfar:
        remote(resx.at[x], resx.at[x], send.at[10], recv.at[10], {"tp": xplus(d)}).start()

    wait_bytes(resx.at[pl.ds(0, NX - 1)], recv.at[10])

    stacked = jnp.concatenate(
        [
            jnp.concatenate([resx[a, :, q * HD : (q + 1) * HD] for a in range(NX)], axis=1)
            for q in range(QB)
        ],
        axis=0,
    )
    sbn[...] = dot(place, stacked, ((0,), (0,))).reshape(NE, RB, NX * HD).astype(BF16)

    for k in direct:
        zt = zplus(NZ - k)
        for i in range(0 if k else 1, NP):
            j, dev = pplus(i)
            remote(sbn.at[zt * NP + j], xn.at[me], send.at[11], recv.at[11], {"ep_0": zt, **dev}).start()
    xn[pl.ds(me, 1)] = sbn[pl.ds(me, 1)]

    for g, ks in enumerate(groups):
        for k in ks:

            zc = pl.multiple_of(zplus(k) * NP, NP)
            wait_bytes(xg.at[0, pl.ds(0, NP)], chunk_recv.at[k])
            for d in xfar:
                remote(
                    xg.at[x, pl.ds(zc, NP)], xg.at[x, pl.ds(zc, NP)],
                    send.at[7], group_recv.at[g], {"tp": xplus(d)},
                ).start()

    slots = NP * CAP
    pr = iota((QB * slots, QB * slots), 0)
    pc = iota((QB * slots, QB * slots), 1)
    to_q = ((lax.rem(pc, QB) == pr // slots) & (pc // QB == lax.rem(pr, slots))).astype(F32).astype(BF16)
    from_q = ((lax.rem(pr, QB) == pc // slots) & (pr // QB == lax.rem(pc, slots))).astype(F32).astype(BF16)
    ld_gf.wait()
    ld_gw.wait()
    ld_uw.wait()
    ld_dw.wait()
    gain = gain_f[...]
    starts = [slots * sum(len(ks) for ks in groups[:g]) for g in range(len(groups))]

    def expert_rows(raw):
        chunks = raw.shape[1] // (NX * HD)
        ordered = dot(to_q, raw)
        res = jnp.concatenate(
            [
                jnp.concatenate(
                    [
                        ordered[q * slots : (q + 1) * slots, (n * NX + a) * HD : (n * NX + a + 1) * HD]
                        for a in range(NX)
                        for q in range(QB)
                    ],
                    axis=1,
                )
                for n in range(chunks)
            ],
            axis=0,
        )
        ffn_in = rms_scale(res, gain).astype(BF16)
        gate_pre = dot(ffn_in, gw[...])
        upward = dot(ffn_in, uw[...])
        capped = jnp.minimum(gate_pre, clamp_limit)
        upward = jnp.clip(upward, -clamp_limit, clamp_limit)
        units = (capped * jax.nn.sigmoid(gate_alpha * capped) * (upward + 1.0)).astype(BF16)
        return units

    def sources(k):
        return pl.ds(pl.multiple_of(zplus(k) * NP, NP), NP)

    def near_experts():

        wait_bytes(xn.at[pl.ds(0, len(direct) * NP - 1)], recv.at[11])

        raw = jnp.concatenate(
            [xn[sources(k)].astype(F32).reshape(NP * RB, NX * HD) for k in direct], axis=1
        ).astype(BF16)
        down = dot(expert_rows(raw), dw[...]).astype(BF16)
        stack = jnp.concatenate(
            [
                jnp.concatenate(
                    [
                        down[n * slots : (n + 1) * slots, a * quarter + q * HD : a * quarter + (q + 1) * HD]
                        for n in range(len(direct))
                        for a in range(NX)
                    ],
                    axis=1,
                )
                for q in range(QB)
            ],
            axis=0,
        )
        back = dot(from_q, stack)
        for n, k in enumerate(direct):
            block = back[:, n * NX * HD : (n + 1) * NX * HD].reshape(NP, RB, NX * HD)
            rbn[sources(k)] = block.astype(BF16)

        for k in direct:
            zc = zplus(k)
            for i in range(0 if k else 1, NP):
                j, dev = pplus(i)
                remote(
                    rbn.at[zc * NP + j], rtn.at[me], send.at[12], recv.at[12], {"ep_0": zc, **dev}
                ).start()
        rtn[pl.ds(me, 1)] = rbn[pl.ds(me, 1)]

    def near_combine():

        wait_bytes(rtn.at[pl.ds(0, len(direct) * NP - 1)], recv.at[12])

        back = rtn[...].astype(F32).reshape(NE * RB, NX * HD).astype(BF16)
        mine = (dot(weight_hi, back) + dot(weight_lo, back)).astype(BF16)
        for a in range(NX):
            nps[a] = mine[:, a * HD : (a + 1) * HD]
        for d in xfar:
            xt = xplus(d)
            remote(nps.at[xt], npr.at[x], send.at[13], recv.at[13], {"tp": xt}).start()
        npr[pl.ds(x, 1)] = nps[pl.ds(x, 1)]

    def experts(g):
        ks = groups[g]
        at = pl.ds(starts[g], slots * len(ks))

        wait_bytes(xg.at[pl.ds(0, NX - 1), pl.ds(0, len(ks) * NP)], group_recv.at[g])

        raw = jnp.concatenate(
            [
                xg[a, sources(k)].astype(F32).reshape(NP * RB, HD)
                for k in ks
                for a in range(NX)
            ],
            axis=1,
        ).astype(BF16)
        down = dot(expert_rows(raw), dw[...]).astype(BF16)
        for q in range(NX):
            epart[q, at] = down[:, q * quarter : (q + 1) * quarter]

        for d in xfar:
            xt = xplus(d)
            remote(epart.at[xt, at], egot.at[x, at], send.at[8], group_got.at[g], {"tp": xt}).start()
        egot[x, at] = epart[x, at]

    def give_back(g):
        ks = groups[g]
        at = pl.ds(starts[g], slots * len(ks))

        wait_bytes(egot.at[pl.ds(0, NX - 1), at], group_got.at[g])

        summed = jnp.sum(egot[:, at].astype(F32), axis=0).astype(BF16)
        stack = jnp.concatenate(
            [
                jnp.concatenate(
                    [summed[n * slots : (n + 1) * slots, q * HD : (q + 1) * HD] for n in range(len(ks))],
                    axis=1,
                )
                for q in range(QB)
            ],
            axis=0,
        )
        back = dot(from_q, stack)
        for n, k in enumerate(ks):
            rb[sources(k)] = back[:, n * HD : (n + 1) * HD].reshape(NP, RB, HD).astype(BF16)

        for k in ks:
            zc = zplus(k)
            for i in range(NP):
                j, dev = pplus(i)
                remote(
                    rb.at[zc * NP + j], rt.at[me], send.at[9], recv.at[9], {"ep_0": zc, **dev}
                ).start()

    G = len(groups)
    for g in range(G):
        experts(g)
    near_experts()
    for g in range(G):
        give_back(g)
    near_combine()

    wait_bytes(got_kv.at[pl.ds(0, NZ - 1)], recv.at[4])
    kv = jnp.sum(got_kv[...].astype(F32), axis=0).astype(BF16)
    new_keys[...] = kv[:, :HD]
    new_values[...] = kv[:, HD:]

    wait_bytes(slices.at[pl.ds(0, NZ - 1)], send.at[0])
    wait_bytes(wq.at[pl.ds(0, NP - 1)], send.at[1])
    wait_bytes(wkv.at[pl.ds(0, NP - 1)], send.at[2])
    wait_bytes(got_q.at[pl.ds(0, NZ - 1)], send.at[3])
    wait_bytes(got_kv.at[pl.ds(0, NZ - 1)], send.at[4])
    wait_bytes(hr.at[pl.ds(0, NX - 1)], send.at[5])
    far_blocks = len(far_ks) * NP
    near_blocks = len(direct) * NP - 1
    wait_bytes(xg.at[0, pl.ds(0, far_blocks)], send.at[6])
    wait_bytes(xg.at[pl.ds(0, NX - 1), pl.ds(0, far_blocks)], send.at[7])
    wait_bytes(egot.at[pl.ds(0, NX - 1), pl.ds(0, far_blocks * CAP)], send.at[8])
    wait_bytes(resx.at[pl.ds(0, NX - 1)], send.at[10])
    wait_bytes(xn.at[pl.ds(0, near_blocks)], send.at[11])
    wait_bytes(rtn.at[pl.ds(0, near_blocks)], send.at[12])
    wait_bytes(npr.at[pl.ds(0, NX - 1)], send.at[13])

    wait_bytes(npr.at[pl.ds(0, NX - 1)], recv.at[13])
    near_sum = jnp.sum(npr[...].astype(F32), axis=0)

    wait_bytes(rt.at[pl.ds(0, far_blocks)], recv.at[9])

    back = rt[...].astype(F32).reshape(NE * RB, HD).astype(BF16)
    routed = near_sum + dot(weight_hi, back) + dot(weight_lo, back)
    res_f = residual.astype(F32)
    for q in range(QB):
        at = slice(q * HD, (q + 1) * HD)
        layer_out[:, at] = (res_f[:, at] + routed[q * seqs : (q + 1) * seqs]).astype(BF16)

    wait_bytes(rt.at[pl.ds(0, far_blocks)], send.at[9])

def tail_kernel(layer_in, keys_in, values_in, layer_out, new_keys, new_values):
    layer_out[...] = layer_in[...]
    new_keys[...] = keys_in[...]
    new_values[...] = values_in[...]

def body(
    tokens, key_cache, value_cache, lengths, attn_gain, query_weight, key_weight, value_weight,
    stay_bias, out_weight, ffn_gain, gate_weight, up_weight, down_weight, routes, route_weight,
):
    routes, route_weight = routes.T, route_weight.T
    sizes = tuple(lax.axis_size(a) for a in AXES)
    NZ, NY, NC, NX = sizes
    NP, NE = NY * NC, NZ * NY * NC
    seqs, width = tokens.shape
    cache_len = key_cache.shape[1]
    quarter = width // NX
    kblock = width // NZ
    QB = quarter // HD
    RB = CAP * QB
    hidden = gate_weight.shape[2]
    G = len(groups_of(list(range(NZ))))
    vm = pltpu.VMEM
    scratch = [
        vm((NX, seqs, quarter), BF16),
        *[vm((NE, RB, NX * HD), BF16)] * 4,
        *[vm((NX, QB * seqs, HD), BF16)] * 2,
        pltpu.SMEM(lengths.shape, jnp.int32), pltpu.SMEM(stay_bias.shape, F32),
        vm((seqs, width), BF16), vm((1, width), F32), vm((1, width), F32),
        vm(routes.shape, jnp.int32), vm(route_weight.shape, F32),
        vm(key_cache.shape, BF16), vm(value_cache.shape, BF16),
        vm(out_weight.shape, BF16), vm((width, hidden), BF16), vm((width, hidden), BF16),
        vm((hidden, width), BF16),
        vm((seqs, width), BF16),
        vm((NZ, seqs, kblock), BF16),
        vm((NP, kblock // NP, 2 * HD), BF16), vm((NP, kblock // NP, 2 * HD), BF16),
        vm((NZ, seqs, 2 * HD), BF16), vm((NZ, seqs, 2 * HD), BF16),
        vm((NZ, seqs, 2 * HD), BF16), vm((NZ, seqs, 2 * HD), BF16),
        vm((2 * seqs, cache_len), BF16),
        vm((NX, seqs, quarter), BF16), vm((NX, seqs, quarter), BF16),
        vm((NE, RB, HD), BF16), vm((NX, NE, RB, HD), BF16),
        vm((NX, NE * CAP, quarter), BF16), vm((NX, NE * CAP, quarter), BF16),
        vm((NE, RB, HD), BF16), vm((NE, RB, HD), BF16),
        pltpu.SemaphoreType.DMA((10,)), pltpu.SemaphoreType.DMA((2, seqs // 2)),
        pltpu.SemaphoreType.DMA((4,)),
        pltpu.SemaphoreType.DMA((14,)), pltpu.SemaphoreType.DMA((14,)),
        pltpu.SemaphoreType.DMA((NZ,)), pltpu.SemaphoreType.DMA((G,)), pltpu.SemaphoreType.DMA((G,)),
    ]
    hbm = pl.BlockSpec(memory_space=pl.ANY)
    in_specs = [hbm] * 16
    shapes = [(seqs, quarter), (seqs, HD), (seqs, HD)]
    out = [jax.ShapeDtypeStruct(shape, BF16) for shape in shapes]
    parts = pl.pallas_call(
        functools.partial(layer_kernel, sizes),
        out_shape=[pltpu.VMEM(shape, BF16) for shape in shapes],
        in_specs=in_specs,
        out_specs=[pl.BlockSpec(memory_space=pltpu.VMEM)] * 3,
        scratch_shapes=scratch,
        compiler_params=pltpu.CompilerParams(
            collective_id=0, has_side_effects=True, vmem_limit_bytes=60 * 1024 * 1024
        ),
    )(
        tokens, key_cache, value_cache, lengths, attn_gain.reshape(1, width), query_weight,
        key_weight, value_weight, stay_bias, out_weight, ffn_gain.reshape(1, width), gate_weight,
        up_weight, down_weight, routes, route_weight,
    )
    vmem = pl.BlockSpec(memory_space=pltpu.VMEM)
    return tuple(pl.pallas_call(
        tail_kernel, out_shape=out, in_specs=[vmem] * 3, out_specs=[vmem] * 3,
        compiler_params=pltpu.CompilerParams(vmem_limit_bytes=1024 * 1024),
    )(*parts))

def solution(mesh):
    finer = Mesh(mesh.devices.reshape(8, 4, 2, mesh.shape["tp"]), AXES)
    placed = (
        P(EP, None), P(EP, None, "tp"), P(EP, None, "tp"), P(EP), P(), P(EP, "tp"), P(EP, "tp"),
        P(EP, "tp"), P("tp"), P("tp", None), P(), P(EP, None, "tp"), P(EP, None, "tp"),
        P(EP, "tp", None), P(EP, None), P(EP, None),
    )
    return jax.shard_map(
        body, mesh=finer, in_specs=placed,
        out_specs=(P(EP, "tp"), P(EP, "tp"), P(EP, "tp")), check_vma=False,
    )
```

```python
import functools
import math

import jax
import jax.numpy as jnp
from jax import lax
from jax.experimental import pallas as pl
from jax.experimental.pallas import tpu as pltpu
from jax.sharding import Mesh
from jax.sharding import PartitionSpec as P

AXES = ("ep_0", "ep_1", "ep_2", "tp")
EP = AXES[:3]
MESH = pl.DeviceIdType.MESH
F32 = jnp.float32
BF16 = jnp.bfloat16
HD = 128
CAP = 2
eps_norm = 1e-05
clamp_limit = 7.0
gate_alpha = 1.702

def dot(a, b, dims=((1,), (0,))):
    return lax.dot_general(a, b, (dims, ((), ())), preferred_element_type=F32)

def rms_scale(values, gain):
    scale = lax.rsqrt(jnp.mean(values * values, axis=-1, keepdims=True) + eps_norm)
    return values * scale * gain

def iota(shape, dim):
    return lax.broadcasted_iota(jnp.int32, shape, dim)

DIRECT = 5

def groups_of(near):
    return [tuple(near[7:]), tuple(near[DIRECT:7])]

def layer_kernel(
    sizes,
    tokens, key_cache, value_cache, lengths_in, attn_gain, query_weight, key_weight, value_weight,
    bias_in, out_weight, ffn_gain, gate_weight, up_weight, down_weight, routes, route_weight,
    layer_out, new_keys, new_values,
    sbn, xn, rbn, rtn, nps, npr, lengths, stay_bias, tok, gain_a, gain_f, route_v, rweight_v, kc, kt, vc, ow, guw, dw,
    normed, slices, wq, wkv, part_q, part_kv, got_q, got_kv,
    sticks, hp, hr, sb, xg, epart, egot, rb, rt,
    loc, kv_sem, exp_sem, send, recv, chunk_recv, group_recv, group_got,
):
    NZ, NY, NC, NX = sizes
    NP = NY * NC
    NE = NZ * NP
    z, y, c, x = (lax.axis_index(a) for a in AXES)
    yc = y * NC + c
    me = z * NP + yc
    seqs, width = tok.shape
    kblock = width // NZ
    quarter = width // NX
    QB = quarter // HD
    cache_len = kc.shape[1]
    RB = CAP * QB
    topk = route_v.shape[0]

    def zplus(d):
        return lax.rem(z + d, NZ)

    plane = []
    for i in range(NP):
        j = lax.rem(yc + i, NP)
        plane.append((j, {"ep_1": j // NC, "ep_2": lax.rem(j, NC)}))

    def pplus(i):
        return plane[i]

    def xplus(d):
        return lax.rem(x + d, NX)

    barrier = pltpu.get_barrier_semaphore()
    for d in range(1, NZ):
        pl.semaphore_signal(barrier, inc=1, device_id={"ep_0": zplus(d)}, device_id_type=MESH)
    for i in range(1, NP):
        pl.semaphore_signal(barrier, inc=1, device_id=pplus(i)[1], device_id_type=MESH)
    for d in range(1, NX):
        pl.semaphore_signal(barrier, inc=1, device_id={"tp": xplus(d)}, device_id_type=MESH)

    def load(src, dst, sem):
        copy = pltpu.make_async_copy(src, dst, sem)
        copy.start()
        return copy

    ld_tok = load(tokens, tok, loc.at[0])
    ld_ga = load(attn_gain, gain_a, loc.at[1])
    ld_wq = load(query_weight, wq.at[yc], loc.at[2])
    ld_wk = load(key_weight, wkv.at[yc, :, pl.ds(0, HD)], loc.at[3])
    ld_wv = load(value_weight, wkv.at[yc, :, pl.ds(HD, HD)], loc.at[4])
    ld_rt = load(routes, route_v, loc.at[5])
    ld_rw = load(route_weight, rweight_v, loc.at[6])
    ld_gf = load(ffn_gain, gain_f, loc.at[7])
    ld_len = load(lengths_in, lengths, loc.at[8])
    ld_bias = load(bias_in, stay_bias, loc.at[9])
    npair = seqs // 2
    ld_k = [load(key_cache.at[pl.ds(2 * p, 2)], kc.at[pl.ds(2 * p, 2)], kv_sem.at[0, p]) for p in range(npair)]
    ld_v = [load(value_cache.at[pl.ds(2 * p, 2)], vc.at[pl.ds(2 * p, 2)], kv_sem.at[1, p]) for p in range(npair)]
    ld_ow = load(out_weight, ow, exp_sem.at[0])
    hidden = dw.shape[0]
    ld_gw = load(gate_weight.at[0], guw.at[:, pl.ds(0, hidden)], exp_sem.at[1])
    ld_uw = load(up_weight.at[0], guw.at[:, pl.ds(hidden, hidden)], exp_sem.at[2])
    ld_dw = load(down_weight.at[0], dw, exp_sem.at[3])

    def remote(src, dst, s, r, device):
        return pltpu.make_async_remote_copy(
            src_ref=src, dst_ref=dst, send_sem=s, recv_sem=r, device_id=device, device_id_type=MESH
        )

    def wait_bytes(ref, sem):
        pltpu.make_async_copy(ref, ref, sem).wait()


    ld_tok.wait()
    ld_ga.wait()
    normed[...] = rms_scale(tok[...].astype(F32), gain_a[...]).astype(BF16)
    ld_wq.wait()

    pl.semaphore_wait(barrier, NZ - 1 + NP - 1 + NX - 1)

    far = sorted(range(1, NZ), key=lambda d: -min(d, NZ - d))
    for d in far:
        zt = zplus(d)
        remote(
            normed.at[:, pl.ds(pl.multiple_of(zt * kblock, kblock), kblock)], slices.at[z],
            send.at[0], recv.at[0], {"ep_0": zt},
        ).start()
    for i in range(1, NP):
        remote(wq.at[yc], wq.at[yc], send.at[1], recv.at[1], pplus(i)[1]).start()
    ld_wk.wait()
    ld_wv.wait()
    for i in range(1, NP):
        remote(wkv.at[yc], wkv.at[yc], send.at[2], recv.at[2], pplus(i)[1]).start()
    slices[pl.ds(z, 1)] = normed[:, pl.ds(pl.multiple_of(z * kblock, kblock), kblock)][None]

    rt[...] = jnp.zeros_like(rt)
    rtn[...] = jnp.zeros_like(rtn)

    def transpose_keys(pairs):
        for p in pairs:
            ld_k[p].wait()
            for s in (2 * p, 2 * p + 1):
                kt[s] = kc[s].T

    transpose_keys(range(npair // 2))

    wait_bytes(slices.at[pl.ds(0, NZ - 1)], recv.at[0])

    wait_bytes(wq.at[pl.ds(0, NP - 1)], recv.at[1])

    lhs = slices[...].reshape(NZ * seqs, kblock)
    part_q[...] = dot(lhs, wq[...].reshape(kblock, 2 * HD)).astype(BF16).reshape(NZ, seqs, 2 * HD)
    for d in far:
        zt = zplus(d)
        remote(part_q.at[zt], got_q.at[z], send.at[3], recv.at[3], {"ep_0": zt}).start()
    got_q[pl.ds(z, 1)] = part_q[pl.ds(z, 1)]

    rows, cols = QB * seqs, NE * RB
    ld_rt.wait()
    ld_rw.wait()
    col = iota((rows, cols), 1)
    row = iota((rows, cols), 0)
    col_e = (col // RB).astype(F32)
    diag = lax.rem(iota((rows, seqs), 0), seqs) == iota((rows, seqs), 1)
    hit = jnp.zeros((rows, cols), F32)
    weighted = jnp.zeros((rows, cols), F32)

    def column(line):
        return jnp.sum(jnp.where(diag, line, 0.0), axis=1, keepdims=True)

    for k in range(topk):
        same = column(route_v[k : k + 1, :].astype(F32)) == col_e
        hit = jnp.where(same, 1.0, hit)
        weighted = jnp.where(same, column(rweight_v[k : k + 1, :]), weighted)
    r0, r1 = iota((rows, rows), 0), iota((rows, rows), 1)
    earlier = ((r0 // seqs == r1 // seqs) & (r1 < r0)).astype(F32).astype(BF16)
    before = dot(earlier, hit.astype(BF16))
    chosen = (row // seqs == lax.rem(col, QB)) & (
        before == (lax.rem(col, RB) // QB).astype(F32)
    )
    place = jnp.where(chosen, hit, 0.0).astype(BF16)
    weighted = jnp.where(chosen, weighted, 0.0)
    weight_hi = weighted.astype(BF16)
    weight_lo = (weighted - weight_hi.astype(F32)).astype(BF16)

    ld_len.wait()
    ld_bias.wait()
    hrow = iota((2 * seqs, 1), 0)
    seq_of = lax.rem(hrow, seqs)
    length_col = jnp.zeros((2 * seqs, 1), jnp.int32)
    for s in range(seqs):
        length_col = jnp.where(seq_of == s, lengths[s], length_col)
    bias_col = jnp.where(hrow < seqs, stay_bias[0], stay_bias[1])

    transpose_keys(range(npair // 2, npair))

    wait_bytes(got_q.at[pl.ds(0, NZ - 1)], recv.at[3])

    query = jnp.sum(got_q[...].astype(F32), axis=0)
    query = jnp.concatenate([query[:, :HD], query[:, HD:]], axis=0).astype(BF16).astype(F32)
    block = jnp.concatenate([jnp.where(seq_of == n, query, 0.0) for n in range(seqs)], axis=1)
    total = dot(block.astype(BF16), kt[...].reshape(seqs * HD, cache_len))

    zs = total * (HD ** -0.5) + bias_col
    live = iota((2 * seqs, cache_len), 1) < length_col
    log_stay = jnp.where(live, -(jnp.maximum(zs, 0.0) + jnp.log1p(jnp.exp(-jnp.abs(zs)))), 0.0)
    blk = min(256, cache_len)
    nblk = cache_len // blk
    n = 2 * seqs
    parts = [log_stay[:, b * blk : (b + 1) * blk] for b in range(nblk)]
    after = [None] * nblk
    for b in reversed(range(nblk - 1)):
        after[b] = parts[b + 1] if after[b + 1] is None else parts[b + 1] + after[b + 1]

    def summed_by(matrix, terms):
        terms = jnp.concatenate(terms, axis=0)
        hi = terms.astype(BF16)
        lo = (terms - hi.astype(F32)).astype(BF16)
        return dot(hi, matrix) + dot(lo, matrix)

    tri = (iota((blk, blk), 0) >= iota((blk, blk), 1)).astype(F32).astype(BF16)
    from_here = summed_by(tri, parts)
    from_later = summed_by(jnp.ones((blk, blk), BF16), after[:-1]) if nblk > 1 else None
    for b in range(nblk):
        at = slice(b * blk, (b + 1) * blk)
        power = zs[:, at] + from_here[b * n : (b + 1) * n]
        if b < nblk - 1:
            power = power + from_later[b * n : (b + 1) * n]
        sticks[:, at] = jnp.where(live[:, at], jnp.exp(power), 0.0).astype(BF16)

    weights = sticks[...]
    att = jnp.zeros((2 * seqs, HD), F32)
    for p in range(npair):
        ld_v[p].wait()
    mixed = dot(weights, jnp.concatenate([vc[n] for n in range(seqs)], axis=1))
    for n in range(seqs):
        att = att + jnp.where(seq_of == n, mixed[:, n * HD : (n + 1) * HD], 0.0)
    att = att.astype(BF16)
    attended = jnp.concatenate([att[:seqs], att[seqs:]], axis=1)

    near = sorted(range(NZ), key=lambda d: (min(d, NZ - d), d))
    groups = groups_of(near)
    direct, far_ks = near[:DIRECT], [k for ks in groups for k in ks]

    ld_ow.wait()
    xfar = sorted(range(1, NX), key=lambda d: -min(d, NX - d))

    hp_full = dot(attended, ow[...]).astype(BF16)
    for q in range(NX):
        hp[q] = hp_full[:, q * quarter : (q + 1) * quarter]

    for d in xfar:
        xt = xplus(d)
        remote(hp.at[xt], hr.at[x, xt], send.at[5], recv.at[5], {"tp": xt}).start()
    for n in range(1, NX):
        for d in xfar:
            xt, q = xplus(d), xplus(d + n)
            remote(hp.at[q], hr.at[x, q], send.at[10], recv.at[10], {"tp": xt}).start()
    hr[pl.ds(x, 1)] = hp[...][None]
    own_tok = tok[:, pl.ds(pl.multiple_of(x * quarter, quarter), quarter)].astype(F32)

    wait_bytes(wkv.at[pl.ds(0, NP - 1)], recv.at[2])

    part_kv[...] = dot(lhs, wkv[...].reshape(kblock, 2 * HD)).astype(BF16).reshape(NZ, seqs, 2 * HD)
    for d in far:
        zt = zplus(d)
        remote(part_kv.at[zt], got_kv.at[z], send.at[4], recv.at[4], {"ep_0": zt}).start()
    got_kv[pl.ds(z, 1)] = part_kv[pl.ds(z, 1)]

    wait_bytes(hr.at[0, pl.ds(0, NX - 1)], recv.at[5])

    residual = (own_tok + jnp.sum(hr[:, pl.ds(x, 1)].astype(F32), axis=(0, 1))).astype(BF16)

    stacked = jnp.concatenate([residual[:, q * HD : (q + 1) * HD] for q in range(QB)], axis=0)
    outgoing = dot(place, stacked, ((0,), (0,)))
    sb[...] = outgoing.reshape(NE, RB, HD).astype(BF16)

    for k in far_ks:
        zt = zplus(NZ - k)
        for i in range(NP):
            j, dev = pplus(i)
            remote(
                sb.at[zt * NP + j], xg.at[x, me], send.at[6], chunk_recv.at[k], {"ep_0": zt, **dev}
            ).start()

    wait_bytes(hr.at[pl.ds(0, NX - 1), pl.ds(0, NX - 1)], recv.at[10])

    rows_of = [
        (
            tok[:, a * quarter : (a + 1) * quarter].astype(F32) + jnp.sum(hr[:, a].astype(F32), axis=0)
        ).astype(BF16)
        for a in range(NX)
    ]
    stacked = jnp.concatenate(
        [
            jnp.concatenate([rows_of[a][:, q * HD : (q + 1) * HD] for a in range(NX)], axis=1)
            for q in range(QB)
        ],
        axis=0,
    )
    sbn[...] = dot(place, stacked, ((0,), (0,))).reshape(NE, RB, NX * HD).astype(BF16)

    for k in direct[::-1]:
        zt = zplus(NZ - k)
        for i in range(0 if k else 1, NP):
            j, dev = pplus(i)
            remote(sbn.at[zt * NP + j], xn.at[me], send.at[11], recv.at[11], {"ep_0": zt, **dev}).start()
    xn[pl.ds(me, 1)] = sbn[pl.ds(me, 1)]

    for g, ks in enumerate(groups):
        for k in ks:

            zc = pl.multiple_of(zplus(k) * NP, NP)
            wait_bytes(xg.at[0, pl.ds(0, NP)], chunk_recv.at[k])
            for d in xfar:
                remote(
                    xg.at[x, pl.ds(zc, NP)], xg.at[x, pl.ds(zc, NP)],
                    send.at[7], group_recv.at[g], {"tp": xplus(d)},
                ).start()

    slots = NP * CAP
    pr = iota((QB * slots, QB * slots), 0)
    pc = iota((QB * slots, QB * slots), 1)
    to_q = ((lax.rem(pc, QB) == pr // slots) & (pc // QB == lax.rem(pr, slots))).astype(F32).astype(BF16)
    from_q = ((lax.rem(pr, QB) == pc // slots) & (pr // QB == lax.rem(pc, slots))).astype(F32).astype(BF16)
    ld_gf.wait()
    ld_gw.wait()
    ld_uw.wait()
    ld_dw.wait()
    gain = gain_f[...]
    starts = [slots * sum(len(ks) for ks in groups[:g]) for g in range(len(groups))]

    def expert_rows(raw):
        chunks = raw.shape[1] // (NX * HD)
        ordered = dot(to_q, raw)
        res = jnp.concatenate(
            [
                jnp.concatenate(
                    [
                        ordered[q * slots : (q + 1) * slots, (n * NX + a) * HD : (n * NX + a + 1) * HD]
                        for a in range(NX)
                        for q in range(QB)
                    ],
                    axis=1,
                )
                for n in range(chunks)
            ],
            axis=0,
        )
        ffn_in = rms_scale(res, gain).astype(BF16)
        both = dot(ffn_in, guw[...])
        capped = jnp.minimum(both[:, :hidden], clamp_limit)
        upward = jnp.clip(both[:, hidden:], -clamp_limit, clamp_limit)
        units = (capped * jax.nn.sigmoid(gate_alpha * capped) * (upward + 1.0)).astype(BF16)
        return units

    def sources(k):
        return pl.ds(pl.multiple_of(zplus(k) * NP, NP), NP)

    def near_experts():

        wait_bytes(xn.at[pl.ds(0, len(direct) * NP - 1)], recv.at[11])

        raw = jnp.concatenate(
            [xn[sources(k)].astype(F32).reshape(NP * RB, NX * HD) for k in direct], axis=1
        ).astype(BF16)
        down = dot(expert_rows(raw), dw[...]).astype(BF16)
        stack = jnp.concatenate(
            [
                jnp.concatenate(
                    [
                        down[n * slots : (n + 1) * slots, a * quarter + q * HD : a * quarter + (q + 1) * HD]
                        for n in range(len(direct))
                        for a in range(NX)
                    ],
                    axis=1,
                )
                for q in range(QB)
            ],
            axis=0,
        )
        back = dot(from_q, stack)
        for n, k in enumerate(direct):
            block = back[:, n * NX * HD : (n + 1) * NX * HD].reshape(NP, RB, NX * HD)
            rbn[sources(k)] = block.astype(BF16)

        for k in direct[::-1]:
            zc = zplus(k)
            for i in range(0 if k else 1, NP):
                j, dev = pplus(i)
                remote(
                    rbn.at[zc * NP + j], rtn.at[me], send.at[12], recv.at[12], {"ep_0": zc, **dev}
                ).start()
        rtn[pl.ds(me, 1)] = rbn[pl.ds(me, 1)]

    def near_combine():

        wait_bytes(rtn.at[pl.ds(0, len(direct) * NP - 1)], recv.at[12])

        back = rtn[...].astype(F32).reshape(NE * RB, NX * HD).astype(BF16)
        mine = (dot(weight_hi, back) + dot(weight_lo, back)).astype(BF16)
        for a in range(NX):
            nps[a] = mine[:, a * HD : (a + 1) * HD]
        for d in xfar:
            xt = xplus(d)
            remote(nps.at[xt], npr.at[x], send.at[13], recv.at[13], {"tp": xt}).start()
        npr[pl.ds(x, 1)] = nps[pl.ds(x, 1)]

    def experts(g):
        ks = groups[g]
        at = pl.ds(starts[g], slots * len(ks))

        wait_bytes(xg.at[pl.ds(0, NX - 1), pl.ds(0, len(ks) * NP)], group_recv.at[g])

        raw = jnp.concatenate(
            [
                xg[a, sources(k)].astype(F32).reshape(NP * RB, HD)
                for k in ks
                for a in range(NX)
            ],
            axis=1,
        ).astype(BF16)
        down = dot(expert_rows(raw), dw[...]).astype(BF16)
        for q in range(NX):
            epart[q, at] = down[:, q * quarter : (q + 1) * quarter]

        for d in xfar:
            xt = xplus(d)
            remote(epart.at[xt, at], egot.at[x, at], send.at[8], group_got.at[g], {"tp": xt}).start()
        egot[x, at] = epart[x, at]

    def give_back(g):
        ks = groups[g]
        at = pl.ds(starts[g], slots * len(ks))

        wait_bytes(egot.at[pl.ds(0, NX - 1), at], group_got.at[g])

        summed = jnp.sum(egot[:, at].astype(F32), axis=0).astype(BF16)
        stack = jnp.concatenate(
            [
                jnp.concatenate(
                    [summed[n * slots : (n + 1) * slots, q * HD : (q + 1) * HD] for n in range(len(ks))],
                    axis=1,
                )
                for q in range(QB)
            ],
            axis=0,
        )
        back = dot(from_q, stack)
        for n, k in enumerate(ks):
            rb[sources(k)] = back[:, n * HD : (n + 1) * HD].reshape(NP, RB, HD).astype(BF16)

        for k in ks:
            zc = zplus(k)
            for i in range(NP):
                j, dev = pplus(i)
                remote(
                    rb.at[zc * NP + j], rt.at[me], send.at[9], recv.at[9], {"ep_0": zc, **dev}
                ).start()

    G = len(groups)
    near_experts()
    for g in range(G):
        experts(g)
    for g in range(G):
        give_back(g)
    near_combine()

    wait_bytes(got_kv.at[pl.ds(0, NZ - 1)], recv.at[4])
    kv = jnp.sum(got_kv[...].astype(F32), axis=0).astype(BF16)
    new_keys[...] = kv[:, :HD]
    new_values[...] = kv[:, HD:]

    wait_bytes(slices.at[pl.ds(0, NZ - 1)], send.at[0])
    wait_bytes(wq.at[pl.ds(0, NP - 1)], send.at[1])
    wait_bytes(wkv.at[pl.ds(0, NP - 1)], send.at[2])
    wait_bytes(got_q.at[pl.ds(0, NZ - 1)], send.at[3])
    wait_bytes(got_kv.at[pl.ds(0, NZ - 1)], send.at[4])
    wait_bytes(hr.at[0, pl.ds(0, NX - 1)], send.at[5])
    far_blocks = len(far_ks) * NP
    near_blocks = len(direct) * NP - 1
    wait_bytes(xg.at[0, pl.ds(0, far_blocks)], send.at[6])
    wait_bytes(xg.at[pl.ds(0, NX - 1), pl.ds(0, far_blocks)], send.at[7])
    wait_bytes(egot.at[pl.ds(0, NX - 1), pl.ds(0, far_blocks * CAP)], send.at[8])
    wait_bytes(hr.at[pl.ds(0, NX - 1), pl.ds(0, NX - 1)], send.at[10])
    wait_bytes(xn.at[pl.ds(0, near_blocks)], send.at[11])
    wait_bytes(rtn.at[pl.ds(0, near_blocks)], send.at[12])
    wait_bytes(npr.at[pl.ds(0, NX - 1)], send.at[13])

    wait_bytes(npr.at[pl.ds(0, NX - 1)], recv.at[13])
    near_sum = jnp.sum(npr[...].astype(F32), axis=0)

    wait_bytes(rt.at[pl.ds(0, far_blocks)], recv.at[9])

    back = rt[...].astype(F32).reshape(NE * RB, HD).astype(BF16)
    routed = near_sum + dot(weight_hi, back) + dot(weight_lo, back)
    res_f = residual.astype(F32)
    for q in range(QB):
        at = slice(q * HD, (q + 1) * HD)
        layer_out[:, at] = (res_f[:, at] + routed[q * seqs : (q + 1) * seqs]).astype(BF16)

    wait_bytes(rt.at[pl.ds(0, far_blocks)], send.at[9])

def tail_kernel(layer_in, keys_in, values_in, layer_out, new_keys, new_values):
    layer_out[...] = layer_in[...]
    new_keys[...] = keys_in[...]
    new_values[...] = values_in[...]

def body(
    tokens, key_cache, value_cache, lengths, attn_gain, query_weight, key_weight, value_weight,
    stay_bias, out_weight, ffn_gain, gate_weight, up_weight, down_weight, routes, route_weight,
):
    routes, route_weight = routes.T, route_weight.T
    sizes = tuple(lax.axis_size(a) for a in AXES)
    NZ, NY, NC, NX = sizes
    NP, NE = NY * NC, NZ * NY * NC
    seqs, width = tokens.shape
    cache_len = key_cache.shape[1]
    quarter = width // NX
    kblock = width // NZ
    QB = quarter // HD
    RB = CAP * QB
    hidden = gate_weight.shape[2]
    G = len(groups_of(list(range(NZ))))
    vm = pltpu.VMEM
    scratch = [
        *[vm((NE, RB, NX * HD), BF16)] * 4,
        *[vm((NX, QB * seqs, HD), BF16)] * 2,
        pltpu.SMEM(lengths.shape, jnp.int32), pltpu.SMEM(stay_bias.shape, F32),
        vm((seqs, width), BF16), vm((1, width), F32), vm((1, width), F32),
        vm(routes.shape, jnp.int32), vm(route_weight.shape, F32),
        vm(key_cache.shape, BF16), vm((seqs, HD, cache_len), BF16), vm(value_cache.shape, BF16),
        vm(out_weight.shape, BF16), vm((width, 2 * hidden), BF16),
        vm((hidden, width), BF16),
        vm((seqs, width), BF16),
        vm((NZ, seqs, kblock), BF16),
        vm((NP, kblock // NP, 2 * HD), BF16), vm((NP, kblock // NP, 2 * HD), BF16),
        vm((NZ, seqs, 2 * HD), BF16), vm((NZ, seqs, 2 * HD), BF16),
        vm((NZ, seqs, 2 * HD), BF16), vm((NZ, seqs, 2 * HD), BF16),
        vm((2 * seqs, cache_len), BF16),
        vm((NX, seqs, quarter), BF16), vm((NX, NX, seqs, quarter), BF16),
        vm((NE, RB, HD), BF16), vm((NX, NE, RB, HD), BF16),
        vm((NX, NE * CAP, quarter), BF16), vm((NX, NE * CAP, quarter), BF16),
        vm((NE, RB, HD), BF16), vm((NE, RB, HD), BF16),
        pltpu.SemaphoreType.DMA((10,)), pltpu.SemaphoreType.DMA((2, seqs // 2)),
        pltpu.SemaphoreType.DMA((4,)),
        pltpu.SemaphoreType.DMA((14,)), pltpu.SemaphoreType.DMA((14,)),
        pltpu.SemaphoreType.DMA((NZ,)), pltpu.SemaphoreType.DMA((G,)), pltpu.SemaphoreType.DMA((G,)),
    ]
    hbm = pl.BlockSpec(memory_space=pl.ANY)
    in_specs = [hbm] * 16
    shapes = [(seqs, quarter), (seqs, HD), (seqs, HD)]
    out = [jax.ShapeDtypeStruct(shape, BF16) for shape in shapes]
    parts = pl.pallas_call(
        functools.partial(layer_kernel, sizes),
        out_shape=[pltpu.VMEM(shape, BF16) for shape in shapes],
        in_specs=in_specs,
        out_specs=[pl.BlockSpec(memory_space=pltpu.VMEM)] * 3,
        scratch_shapes=scratch,
        compiler_params=pltpu.CompilerParams(
            collective_id=0, has_side_effects=True, vmem_limit_bytes=60 * 1024 * 1024
        ),
    )(
        tokens, key_cache, value_cache, lengths, attn_gain.reshape(1, width), query_weight,
        key_weight, value_weight, stay_bias, out_weight, ffn_gain.reshape(1, width), gate_weight,
        up_weight, down_weight, routes, route_weight,
    )
    vmem = pl.BlockSpec(memory_space=pltpu.VMEM)
    return tuple(pl.pallas_call(
        tail_kernel, out_shape=out, in_specs=[vmem] * 3, out_specs=[vmem] * 3,
        compiler_params=pltpu.CompilerParams(vmem_limit_bytes=1024 * 1024),
    )(*parts))

def solution(mesh):
    finer = Mesh(mesh.devices.reshape(8, 4, 2, mesh.shape["tp"]), AXES)
    placed = (
        P(EP, None), P(EP, None, "tp"), P(EP, None, "tp"), P(EP), P(), P(EP, "tp"), P(EP, "tp"),
        P(EP, "tp"), P("tp"), P("tp", None), P(), P(EP, None, "tp"), P(EP, None, "tp"),
        P(EP, "tp", None), P(EP, None), P(EP, None),
    )
    return jax.shard_map(
        body, mesh=finer, in_specs=placed,
        out_specs=(P(EP, "tp"), P(EP, "tp"), P(EP, "tp")), check_vma=False,
    )
```

```python
import functools
import math

import jax
import jax.numpy as jnp
from jax import lax
from jax.experimental import pallas as pl
from jax.experimental.pallas import tpu as pltpu
from jax.sharding import Mesh
from jax.sharding import PartitionSpec as P

AXES = ("ep_0", "ep_1", "ep_2", "tp")
EP = AXES[:3]
MESH = pl.DeviceIdType.MESH
F32 = jnp.float32
BF16 = jnp.bfloat16
HD = 128
CAP = 2
eps_norm = 1e-05
clamp_limit = 7.0
gate_alpha = 1.702

def dot(a, b, dims=((1,), (0,))):
    return lax.dot_general(a, b, (dims, ((), ())), preferred_element_type=F32)

def rms_scale(values, gain):
    scale = lax.rsqrt(jnp.mean(values * values, axis=-1, keepdims=True) + eps_norm)
    return values * scale * gain

def iota(shape, dim):
    return lax.broadcasted_iota(jnp.int32, shape, dim)

DIRECT = 5

def groups_of(near):
    return [tuple(near[7:]), tuple(near[DIRECT:7])]

def layer_kernel(
    sizes,
    tokens, key_cache, value_cache, lengths_in, attn_gain, query_weight, key_weight, value_weight,
    bias_in, out_weight, ffn_gain, gate_weight, up_weight, down_weight, routes, route_weight,
    layer_out, new_keys, new_values,
    place, sbn, xn, rbn, rtn, nps, npr, lengths, stay_bias, tok, gain_a, gain_f, route_v, rweight_v, kc, kt, vc, ow, guw, dw,
    normed, slices, wq, wkv, part_q, part_kv, got_q, got_kv,
    sticks, hp, hr, sb, xg, epart, egot, rb, rt,
    loc, kv_sem, exp_sem, send, recv, chunk_recv, group_recv, group_got,
):
    NZ, NY, NC, NX = sizes
    NP = NY * NC
    NE = NZ * NP
    z, y, c, x = (lax.axis_index(a) for a in AXES)
    yc = y * NC + c
    me = z * NP + yc
    seqs, width = tok.shape
    kblock = width // NZ
    quarter = width // NX
    QB = quarter // HD
    cache_len = kc.shape[1]
    RB = CAP * QB
    topk = route_v.shape[0]

    def zplus(d):
        return lax.rem(z + d, NZ)

    plane = []
    for i in range(NP):
        j = lax.rem(yc + i, NP)
        plane.append((j, {"ep_1": j // NC, "ep_2": lax.rem(j, NC)}))

    def pplus(i):
        return plane[i]

    def xplus(d):
        return lax.rem(x + d, NX)

    barrier = pltpu.get_barrier_semaphore()
    for d in range(1, NZ):
        pl.semaphore_signal(barrier, inc=1, device_id={"ep_0": zplus(d)}, device_id_type=MESH)
    for i in range(1, NP):
        pl.semaphore_signal(barrier, inc=1, device_id=pplus(i)[1], device_id_type=MESH)
    for d in range(1, NX):
        pl.semaphore_signal(barrier, inc=1, device_id={"tp": xplus(d)}, device_id_type=MESH)

    def load(src, dst, sem):
        copy = pltpu.make_async_copy(src, dst, sem)
        copy.start()
        return copy

    ld_tok = load(tokens, tok, loc.at[0])
    ld_ga = load(attn_gain, gain_a, loc.at[1])
    ld_wq = load(query_weight, wq.at[yc], loc.at[2])
    ld_wk = load(key_weight, wkv.at[yc, :, pl.ds(0, HD)], loc.at[3])
    ld_wv = load(value_weight, wkv.at[yc, :, pl.ds(HD, HD)], loc.at[4])
    ld_rt = load(routes, route_v, loc.at[5])
    ld_rw = load(route_weight, rweight_v, loc.at[6])
    ld_gf = load(ffn_gain, gain_f, loc.at[7])
    ld_len = load(lengths_in, lengths, loc.at[8])
    ld_bias = load(bias_in, stay_bias, loc.at[9])
    npair = seqs // 2
    ld_k = [load(key_cache.at[pl.ds(2 * p, 2)], kc.at[pl.ds(2 * p, 2)], kv_sem.at[0, p]) for p in range(npair)]
    ld_v = [load(value_cache.at[pl.ds(2 * p, 2)], vc.at[pl.ds(2 * p, 2)], kv_sem.at[1, p]) for p in range(npair)]
    ld_ow = load(out_weight, ow, exp_sem.at[0])
    hidden = dw.shape[0]
    ld_gw = load(gate_weight.at[0], guw.at[:, pl.ds(0, hidden)], exp_sem.at[1])
    ld_uw = load(up_weight.at[0], guw.at[:, pl.ds(hidden, hidden)], exp_sem.at[2])
    ld_dw = load(down_weight.at[0], dw, exp_sem.at[3])

    def remote(src, dst, s, r, device):
        return pltpu.make_async_remote_copy(
            src_ref=src, dst_ref=dst, send_sem=s, recv_sem=r, device_id=device, device_id_type=MESH
        )

    def wait_bytes(ref, sem):
        pltpu.make_async_copy(ref, ref, sem).wait()


    ld_tok.wait()
    ld_ga.wait()
    normed[...] = rms_scale(tok[...].astype(F32), gain_a[...]).astype(BF16)
    ld_wq.wait()

    pl.semaphore_wait(barrier, NZ - 1 + NP - 1 + NX - 1)

    far = sorted(range(1, NZ), key=lambda d: -min(d, NZ - d))
    for d in far:
        zt = zplus(d)
        remote(
            normed.at[:, pl.ds(pl.multiple_of(zt * kblock, kblock), kblock)], slices.at[z],
            send.at[0], recv.at[0], {"ep_0": zt},
        ).start()
    for i in range(1, NP):
        remote(wq.at[yc], wq.at[yc], send.at[1], recv.at[1], pplus(i)[1]).start()
    slices[pl.ds(z, 1)] = normed[:, pl.ds(pl.multiple_of(z * kblock, kblock), kblock)][None]

    rt[...] = jnp.zeros_like(rt)
    rtn[...] = jnp.zeros_like(rtn)

    def transpose_keys(pairs):
        for p in pairs:
            ld_k[p].wait()
            for s in (2 * p, 2 * p + 1):
                kt[s] = kc[s].T

    transpose_keys(range(npair // 2))

    wait_bytes(slices.at[pl.ds(0, NZ - 1)], recv.at[0])

    wait_bytes(wq.at[pl.ds(0, NP - 1)], recv.at[1])

    lhs = slices[...].reshape(NZ * seqs, kblock)
    part_q[...] = dot(lhs, wq[...].reshape(kblock, 2 * HD)).astype(BF16).reshape(NZ, seqs, 2 * HD)
    for d in far:
        zt = zplus(d)
        remote(part_q.at[zt], got_q.at[z], send.at[3], recv.at[3], {"ep_0": zt}).start()
    got_q[pl.ds(z, 1)] = part_q[pl.ds(z, 1)]

    ld_wk.wait()
    ld_wv.wait()
    for i in range(1, NP):
        remote(wkv.at[yc], wkv.at[yc], send.at[2], recv.at[2], pplus(i)[1]).start()

    rows, cols = QB * seqs, NE * RB
    ld_rt.wait()
    ld_rw.wait()
    col = iota((rows, cols), 1)
    row = iota((rows, cols), 0)
    col_e = (col // RB).astype(F32)
    diag = lax.rem(iota((rows, seqs), 0), seqs) == iota((rows, seqs), 1)
    hit = jnp.zeros((rows, cols), F32)
    weighted = jnp.zeros((rows, cols), F32)

    def column(line):
        return jnp.sum(jnp.where(diag, line, 0.0), axis=1, keepdims=True)

    for k in range(topk):
        same = column(route_v[k : k + 1, :].astype(F32)) == col_e
        hit = jnp.where(same, 1.0, hit)
        weighted = jnp.where(same, column(rweight_v[k : k + 1, :]), weighted)
    r0, r1 = iota((rows, rows), 0), iota((rows, rows), 1)
    earlier = ((r0 // seqs == r1 // seqs) & (r1 < r0)).astype(F32).astype(BF16)
    before = dot(earlier, hit.astype(BF16))
    chosen = (row // seqs == lax.rem(col, QB)) & (
        before == (lax.rem(col, RB) // QB).astype(F32)
    )
    place[...] = jnp.where(chosen, hit, 0.0).T.astype(BF16)
    weighted = jnp.where(chosen, weighted, 0.0)
    weight_hi = weighted.astype(BF16)
    weight_lo = (weighted - weight_hi.astype(F32)).astype(BF16)

    ld_len.wait()
    ld_bias.wait()
    hrow = iota((2 * seqs, 1), 0)
    seq_of = lax.rem(hrow, seqs)
    length_col = jnp.zeros((2 * seqs, 1), jnp.int32)
    for s in range(seqs):
        length_col = jnp.where(seq_of == s, lengths[s], length_col)
    bias_col = jnp.where(hrow < seqs, stay_bias[0], stay_bias[1])

    transpose_keys(range(npair // 2, npair))

    wait_bytes(got_q.at[pl.ds(0, NZ - 1)], recv.at[3])

    query = jnp.sum(got_q[...].astype(F32), axis=0)
    query = jnp.concatenate([query[:, :HD], query[:, HD:]], axis=0).astype(BF16).astype(F32)
    block = jnp.concatenate([jnp.where(seq_of == n, query, 0.0) for n in range(seqs)], axis=1)
    total = dot(block.astype(BF16), kt[...].reshape(seqs * HD, cache_len))

    zs = total * (HD ** -0.5) + bias_col
    live = iota((2 * seqs, cache_len), 1) < length_col
    rest = jnp.log1p(jnp.exp(-jnp.abs(zs)))
    log_stay = jnp.where(live, -(jnp.maximum(zs, 0.0) + rest), 0.0)
    log_break = jnp.minimum(zs, 0.0) - rest
    blk = min(256, cache_len)
    nblk = cache_len // blk
    n = 2 * seqs
    parts = [log_stay[:, b * blk : (b + 1) * blk] for b in range(nblk)]
    after = [None] * nblk
    for b in reversed(range(nblk - 1)):
        after[b] = parts[b + 1] if after[b + 1] is None else parts[b + 1] + after[b + 1]

    def summed_by(matrix, terms):
        terms = jnp.concatenate(terms, axis=0)
        hi = terms.astype(BF16)
        lo = (terms - hi.astype(F32)).astype(BF16)
        return dot(hi, matrix) + dot(lo, matrix)

    tri = (iota((blk, blk), 0) > iota((blk, blk), 1)).astype(F32).astype(BF16)
    in_block = summed_by(tri, parts)
    in_later = summed_by(jnp.ones((blk, blk), BF16), after[:-1]) if nblk > 1 else None
    for b in range(nblk):
        at = slice(b * blk, (b + 1) * blk)
        power = log_break[:, at] + in_block[b * n : (b + 1) * n]
        if b < nblk - 1:
            power = power + in_later[b * n : (b + 1) * n]
        sticks[:, at] = jnp.where(live[:, at], jnp.exp(power), 0.0).astype(BF16)

    weights = sticks[...]
    att = jnp.zeros((2 * seqs, HD), F32)
    for p in range(npair):
        ld_v[p].wait()
    mixed = dot(weights, jnp.concatenate([vc[n] for n in range(seqs)], axis=1))
    for n in range(seqs):
        att = att + jnp.where(seq_of == n, mixed[:, n * HD : (n + 1) * HD], 0.0)
    att = att.astype(BF16)
    attended = jnp.concatenate([att[:seqs], att[seqs:]], axis=1)

    near = sorted(range(NZ), key=lambda d: (min(d, NZ - d), d))
    groups = groups_of(near)
    direct, far_ks = near[:DIRECT], [k for ks in groups for k in ks]

    ld_ow.wait()
    xfar = sorted(range(1, NX), key=lambda d: -min(d, NX - d))

    hp_full = dot(attended, ow[...]).astype(BF16)
    for q in range(NX):
        hp[q] = hp_full[:, q * quarter : (q + 1) * quarter]

    for d in xfar:
        xt = xplus(d)
        remote(hp.at[xt], hr.at[x, xt], send.at[5], recv.at[5], {"tp": xt}).start()
    for n in range(1, NX):
        for d in xfar:
            xt, q = xplus(d), xplus(d + n)
            remote(hp.at[q], hr.at[x, q], send.at[10], recv.at[10], {"tp": xt}).start()
    hr[pl.ds(x, 1)] = hp[...][None]
    own_tok = tok[:, pl.ds(pl.multiple_of(x * quarter, quarter), quarter)].astype(F32)

    wait_bytes(wkv.at[pl.ds(0, NP - 1)], recv.at[2])

    part_kv[...] = dot(lhs, wkv[...].reshape(kblock, 2 * HD)).astype(BF16).reshape(NZ, seqs, 2 * HD)
    for d in far:
        zt = zplus(d)
        remote(part_kv.at[zt], got_kv.at[z], send.at[4], recv.at[4], {"ep_0": zt}).start()
    got_kv[pl.ds(z, 1)] = part_kv[pl.ds(z, 1)]

    wait_bytes(hr.at[0, pl.ds(0, NX - 1)], recv.at[5])

    residual = (own_tok + jnp.sum(hr[:, pl.ds(x, 1)].astype(F32), axis=(0, 1))).astype(BF16)

    stacked = jnp.concatenate([residual[:, q * HD : (q + 1) * HD] for q in range(QB)], axis=0)
    outgoing = dot(place[...], stacked)
    sb[...] = outgoing.reshape(NE, RB, HD).astype(BF16)

    for k in far_ks:
        zt = zplus(NZ - k)
        for i in range(NP):
            j, dev = pplus(i)
            remote(
                sb.at[zt * NP + j], xg.at[x, me], send.at[6], chunk_recv.at[k], {"ep_0": zt, **dev}
            ).start()

    wait_bytes(hr.at[pl.ds(0, NX - 1), pl.ds(0, NX - 1)], recv.at[10])

    rows_of = [
        (
            tok[:, a * quarter : (a + 1) * quarter].astype(F32) + jnp.sum(hr[:, a].astype(F32), axis=0)
        ).astype(BF16)
        for a in range(NX)
    ]
    stacked = jnp.concatenate(
        [
            jnp.concatenate([rows_of[a][:, q * HD : (q + 1) * HD] for a in range(NX)], axis=1)
            for q in range(QB)
        ],
        axis=0,
    )
    sbn[...] = dot(place[...], stacked).reshape(NE, RB, NX * HD).astype(BF16)

    for k in direct[::-1]:
        zt = zplus(NZ - k)
        for i in range(0 if k else 1, NP):
            j, dev = pplus(i)
            remote(sbn.at[zt * NP + j], xn.at[me], send.at[11], recv.at[11], {"ep_0": zt, **dev}).start()
    xn[pl.ds(me, 1)] = sbn[pl.ds(me, 1)]

    for g, ks in enumerate(groups):
        for k in ks:

            zc = pl.multiple_of(zplus(k) * NP, NP)
            wait_bytes(xg.at[0, pl.ds(0, NP)], chunk_recv.at[k])
            for d in xfar:
                remote(
                    xg.at[x, pl.ds(zc, NP)], xg.at[x, pl.ds(zc, NP)],
                    send.at[7], group_recv.at[g], {"tp": xplus(d)},
                ).start()

    slots = NP * CAP
    pr = iota((QB * slots, QB * slots), 0)
    pc = iota((QB * slots, QB * slots), 1)
    to_q = ((lax.rem(pc, QB) == pr // slots) & (pc // QB == lax.rem(pr, slots))).astype(F32).astype(BF16)
    from_q = ((lax.rem(pr, QB) == pc // slots) & (pr // QB == lax.rem(pc, slots))).astype(F32).astype(BF16)
    ld_gf.wait()
    ld_gw.wait()
    ld_uw.wait()
    ld_dw.wait()
    gain = gain_f[...]
    starts = [slots * sum(len(ks) for ks in groups[:g]) for g in range(len(groups))]

    def expert_rows(raw):
        chunks = raw.shape[1] // (NX * HD)
        ordered = dot(to_q, raw)
        res = jnp.concatenate(
            [
                jnp.concatenate(
                    [
                        ordered[q * slots : (q + 1) * slots, (n * NX + a) * HD : (n * NX + a + 1) * HD]
                        for a in range(NX)
                        for q in range(QB)
                    ],
                    axis=1,
                )
                for n in range(chunks)
            ],
            axis=0,
        )
        ffn_in = rms_scale(res, gain).astype(BF16)
        both = dot(ffn_in, guw[...])
        capped = jnp.minimum(both[:, :hidden], clamp_limit)
        upward = jnp.clip(both[:, hidden:], -clamp_limit, clamp_limit)
        units = (capped * jax.nn.sigmoid(gate_alpha * capped) * (upward + 1.0)).astype(BF16)
        return units

    def sources(k):
        return pl.ds(pl.multiple_of(zplus(k) * NP, NP), NP)

    def near_experts():

        wait_bytes(xn.at[pl.ds(0, len(direct) * NP - 1)], recv.at[11])

        raw = jnp.concatenate(
            [xn[sources(k)].astype(F32).reshape(NP * RB, NX * HD) for k in direct], axis=1
        ).astype(BF16)
        down = dot(expert_rows(raw), dw[...]).astype(BF16)
        stack = jnp.concatenate(
            [
                jnp.concatenate(
                    [
                        down[n * slots : (n + 1) * slots, a * quarter + q * HD : a * quarter + (q + 1) * HD]
                        for n in range(len(direct))
                        for a in range(NX)
                    ],
                    axis=1,
                )
                for q in range(QB)
            ],
            axis=0,
        )
        back = dot(from_q, stack)
        for n, k in enumerate(direct):
            block = back[:, n * NX * HD : (n + 1) * NX * HD].reshape(NP, RB, NX * HD)
            rbn[sources(k)] = block.astype(BF16)

        for k in direct[::-1]:
            zc = zplus(k)
            for i in range(0 if k else 1, NP):
                j, dev = pplus(i)
                remote(
                    rbn.at[zc * NP + j], rtn.at[me], send.at[12], recv.at[12], {"ep_0": zc, **dev}
                ).start()
        rtn[pl.ds(me, 1)] = rbn[pl.ds(me, 1)]

    def near_combine():

        wait_bytes(rtn.at[pl.ds(0, len(direct) * NP - 1)], recv.at[12])

        back = rtn[...].astype(F32).reshape(NE * RB, NX * HD).astype(BF16)
        mine = (dot(weight_hi, back) + dot(weight_lo, back)).astype(BF16)
        for a in range(NX):
            nps[a] = mine[:, a * HD : (a + 1) * HD]
        for d in xfar:
            xt = xplus(d)
            remote(nps.at[xt], npr.at[x], send.at[13], recv.at[13], {"tp": xt}).start()
        npr[pl.ds(x, 1)] = nps[pl.ds(x, 1)]

    def experts(g):
        ks = groups[g]
        at = pl.ds(starts[g], slots * len(ks))

        wait_bytes(xg.at[pl.ds(0, NX - 1), pl.ds(0, len(ks) * NP)], group_recv.at[g])

        raw = jnp.concatenate(
            [
                xg[a, sources(k)].astype(F32).reshape(NP * RB, HD)
                for k in ks
                for a in range(NX)
            ],
            axis=1,
        ).astype(BF16)
        down = dot(expert_rows(raw), dw[...]).astype(BF16)
        for q in range(NX):
            epart[q, at] = down[:, q * quarter : (q + 1) * quarter]

        for d in xfar:
            xt = xplus(d)
            remote(epart.at[xt, at], egot.at[x, at], send.at[8], group_got.at[g], {"tp": xt}).start()
        egot[x, at] = epart[x, at]

    def give_back(g):
        ks = groups[g]
        at = pl.ds(starts[g], slots * len(ks))

        wait_bytes(egot.at[pl.ds(0, NX - 1), at], group_got.at[g])

        summed = jnp.sum(egot[:, at].astype(F32), axis=0).astype(BF16)
        stack = jnp.concatenate(
            [
                jnp.concatenate(
                    [summed[n * slots : (n + 1) * slots, q * HD : (q + 1) * HD] for n in range(len(ks))],
                    axis=1,
                )
                for q in range(QB)
            ],
            axis=0,
        )
        back = dot(from_q, stack)
        for n, k in enumerate(ks):
            rb[sources(k)] = back[:, n * HD : (n + 1) * HD].reshape(NP, RB, HD).astype(BF16)

        for k in ks:
            zc = zplus(k)
            for i in range(NP):
                j, dev = pplus(i)
                remote(
                    rb.at[zc * NP + j], rt.at[me], send.at[9], recv.at[9], {"ep_0": zc, **dev}
                ).start()

    G = len(groups)
    near_experts()
    for g in range(G):
        experts(g)
    for g in range(G):
        give_back(g)
    near_combine()

    wait_bytes(got_kv.at[pl.ds(0, NZ - 1)], recv.at[4])
    kv = jnp.sum(got_kv[...].astype(F32), axis=0).astype(BF16)
    new_keys[...] = kv[:, :HD]
    new_values[...] = kv[:, HD:]

    far_blocks = len(far_ks) * NP
    near_blocks = len(direct) * NP - 1

    wait_bytes(npr.at[pl.ds(0, NX - 1)], recv.at[13])
    near_sum = jnp.sum(npr[...].astype(F32), axis=0)

    wait_bytes(rt.at[pl.ds(0, far_blocks)], recv.at[9])

    back = rt[...].astype(F32).reshape(NE * RB, HD).astype(BF16)
    routed = near_sum + dot(weight_hi, back) + dot(weight_lo, back)
    res_f = residual.astype(F32)
    for q in range(QB):
        at = slice(q * HD, (q + 1) * HD)
        layer_out[:, at] = (res_f[:, at] + routed[q * seqs : (q + 1) * seqs]).astype(BF16)

    wait_bytes(slices.at[pl.ds(0, NZ - 1)], send.at[0])
    wait_bytes(wq.at[pl.ds(0, NP - 1)], send.at[1])
    wait_bytes(wkv.at[pl.ds(0, NP - 1)], send.at[2])
    wait_bytes(got_q.at[pl.ds(0, NZ - 1)], send.at[3])
    wait_bytes(got_kv.at[pl.ds(0, NZ - 1)], send.at[4])
    wait_bytes(hr.at[0, pl.ds(0, NX - 1)], send.at[5])
    wait_bytes(xg.at[0, pl.ds(0, far_blocks)], send.at[6])
    wait_bytes(xg.at[pl.ds(0, NX - 1), pl.ds(0, far_blocks)], send.at[7])
    wait_bytes(egot.at[pl.ds(0, NX - 1), pl.ds(0, far_blocks * CAP)], send.at[8])
    wait_bytes(hr.at[pl.ds(0, NX - 1), pl.ds(0, NX - 1)], send.at[10])
    wait_bytes(xn.at[pl.ds(0, near_blocks)], send.at[11])
    wait_bytes(rtn.at[pl.ds(0, near_blocks)], send.at[12])
    wait_bytes(npr.at[pl.ds(0, NX - 1)], send.at[13])
    wait_bytes(rt.at[pl.ds(0, far_blocks)], send.at[9])

def tail_kernel(layer_in, keys_in, values_in, layer_out, new_keys, new_values):
    layer_out[...] = layer_in[...]
    new_keys[...] = keys_in[...]
    new_values[...] = values_in[...]

def body(
    tokens, key_cache, value_cache, lengths, attn_gain, query_weight, key_weight, value_weight,
    stay_bias, out_weight, ffn_gain, gate_weight, up_weight, down_weight, routes, route_weight,
):
    routes, route_weight = routes.T, route_weight.T
    sizes = tuple(lax.axis_size(a) for a in AXES)
    NZ, NY, NC, NX = sizes
    NP, NE = NY * NC, NZ * NY * NC
    seqs, width = tokens.shape
    cache_len = key_cache.shape[1]
    quarter = width // NX
    kblock = width // NZ
    QB = quarter // HD
    RB = CAP * QB
    hidden = gate_weight.shape[2]
    G = len(groups_of(list(range(NZ))))
    vm = pltpu.VMEM
    scratch = [
        vm((NE * RB, QB * seqs), BF16),
        *[vm((NE, RB, NX * HD), BF16)] * 4,
        *[vm((NX, QB * seqs, HD), BF16)] * 2,
        pltpu.SMEM(lengths.shape, jnp.int32), pltpu.SMEM(stay_bias.shape, F32),
        vm((seqs, width), BF16), vm((1, width), F32), vm((1, width), F32),
        vm(routes.shape, jnp.int32), vm(route_weight.shape, F32),
        vm(key_cache.shape, BF16), vm((seqs, HD, cache_len), BF16), vm(value_cache.shape, BF16),
        vm(out_weight.shape, BF16), vm((width, 2 * hidden), BF16),
        vm((hidden, width), BF16),
        vm((seqs, width), BF16),
        vm((NZ, seqs, kblock), BF16),
        vm((NP, kblock // NP, 2 * HD), BF16), vm((NP, kblock // NP, 2 * HD), BF16),
        vm((NZ, seqs, 2 * HD), BF16), vm((NZ, seqs, 2 * HD), BF16),
        vm((NZ, seqs, 2 * HD), BF16), vm((NZ, seqs, 2 * HD), BF16),
        vm((2 * seqs, cache_len), BF16),
        vm((NX, seqs, quarter), BF16), vm((NX, NX, seqs, quarter), BF16),
        vm((NE, RB, HD), BF16), vm((NX, NE, RB, HD), BF16),
        vm((NX, NE * CAP, quarter), BF16), vm((NX, NE * CAP, quarter), BF16),
        vm((NE, RB, HD), BF16), vm((NE, RB, HD), BF16),
        pltpu.SemaphoreType.DMA((10,)), pltpu.SemaphoreType.DMA((2, seqs // 2)),
        pltpu.SemaphoreType.DMA((4,)),
        pltpu.SemaphoreType.DMA((14,)), pltpu.SemaphoreType.DMA((14,)),
        pltpu.SemaphoreType.DMA((NZ,)), pltpu.SemaphoreType.DMA((G,)), pltpu.SemaphoreType.DMA((G,)),
    ]
    hbm = pl.BlockSpec(memory_space=pl.ANY)
    in_specs = [hbm] * 16
    shapes = [(seqs, quarter), (seqs, HD), (seqs, HD)]
    out = [jax.ShapeDtypeStruct(shape, BF16) for shape in shapes]
    parts = pl.pallas_call(
        functools.partial(layer_kernel, sizes),
        out_shape=[pltpu.VMEM(shape, BF16) for shape in shapes],
        in_specs=in_specs,
        out_specs=[pl.BlockSpec(memory_space=pltpu.VMEM)] * 3,
        scratch_shapes=scratch,
        compiler_params=pltpu.CompilerParams(
            collective_id=0, has_side_effects=True, vmem_limit_bytes=60 * 1024 * 1024
        ),
    )(
        tokens, key_cache, value_cache, lengths, attn_gain.reshape(1, width), query_weight,
        key_weight, value_weight, stay_bias, out_weight, ffn_gain.reshape(1, width), gate_weight,
        up_weight, down_weight, routes, route_weight,
    )
    vmem = pl.BlockSpec(memory_space=pltpu.VMEM)
    return tuple(pl.pallas_call(
        tail_kernel, out_shape=out, in_specs=[vmem] * 3, out_specs=[vmem] * 3,
        compiler_params=pltpu.CompilerParams(vmem_limit_bytes=1024 * 1024),
    )(*parts))

def solution(mesh):
    finer = Mesh(mesh.devices.reshape(8, 4, 2, mesh.shape["tp"]), AXES)
    placed = (
        P(EP, None), P(EP, None, "tp"), P(EP, None, "tp"), P(EP), P(), P(EP, "tp"), P(EP, "tp"),
        P(EP, "tp"), P("tp"), P("tp", None), P(), P(EP, None, "tp"), P(EP, None, "tp"),
        P(EP, "tp", None), P(EP, None), P(EP, None),
    )
    return jax.shard_map(
        body, mesh=finer, in_specs=placed,
        out_specs=(P(EP, "tp"), P(EP, "tp"), P(EP, "tp")), check_vma=False,
    )
```
